512 devices in a mesh: grp: 2 (over y), sp: 64 (over z, core), tp: 4 (over x).
Axes of the slice: x: 4, y: 2, z: 32, core: 2. Of those that a mesh axis runs over, the one named last changes fastest.
The devices are a block of a 4x8x32 slice.
Arguments:
- tokens: bfloat16 [16384, 2048], P(('grp', 'sp'), 'tp'), parts along dimension 0
- mix_gain: bfloat16 [2048], replicated, may hold values from 0.099609375 to 1.8984375
- w_conv_value: bfloat16 [2048, 1024], P('sp', 'tp'), may hold values from -0.125 to 0.125
- w_conv_outer: bfloat16 [2048, 1024], P('sp', 'tp'), may hold values from -0.125 to 0.125
- w_conv_inner: bfloat16 [2048, 1024], P('sp', 'tp'), may hold values from -0.125 to 0.125
- conv_kernel: bfloat16 [3, 1024], P(None, 'tp'), may hold values from -3.5 to 3.5
- w_q_down: bfloat16 [2048, 512], P(None, 'tp'), may hold values from -0.125 to 0.125
- w_kv_down: bfloat16 [2048, 256], P(None, 'tp'), may hold values from -0.125 to 0.125
- w_rope_key: bfloat16 [2048, 32], replicated, may hold values from -0.125 to 0.125
- q_gain: bfloat16 [512], replicated
- kv_gain: bfloat16 [256], replicated, may hold values from 0.099609375 to 1.8984375
- w_q_nope: bfloat16 [512, 1024], P(None, 'tp'), may hold values from -0.25 to 0.25
- w_q_rope: bfloat16 [512, 512], P(None, 'tp'), may hold values from -0.25 to 0.25
- w_k_nope: bfloat16 [256, 1024], P(None, 'tp'), may hold values from -0.375 to 0.375
- w_value: bfloat16 [256, 1024], P(None, 'tp'), may hold values from -0.375 to 0.375
- w_out_conv: bfloat16 [1024, 2048], P('tp'), may hold values from -0.1875 to 0.1875
- w_out_attn: bfloat16 [1024, 2048], P('tp'), may hold values from -1.5 to 1.5
Outputs:
- mixed: bfloat16 [16384, 2048], P(('grp', 'sp'), 'tp'), parts along dimension 0
The draws below stay inside these ranges and needn't reach their ends.
There are 2 independent parts, one for each index of `grp`. The reference program is written for one: setup_inputs(seed, part) draws one part's arguments, and reference() takes and returns one part's arrays. A program takes and returns all parts, laid end to end along the dimension named above; an argument that names none is the same for every part. Nothing has to cross between parts.
All inputs are finite; a program needn't handle non-finite values.
Results may differ from the reference program's by a relative error of at most 0.028.
Values may be sent and summed in bfloat16 or wider, within the bound.
A program may use at most 64 MiB of HBM per device.

```python
import jax
import jax.numpy as jnp
from jax import lax

D = 2048
MLA_HEADS = 16
Q_LATENT = 512
KV_LATENT = 256
NOPE = 64
ROPE = 32
VALUE = 64
TAPS = 3
TOKENS = 8192
CONV_WIDTH = 1024
N_TP = 4


def draw_tokens(key, part):
    first = jax.random.fold_in(key, 11)
    second = jax.random.fold_in(key, 12)
    column = jnp.arange(D, dtype=jnp.float32) / max(D - 1, 1)
    column_scale = jnp.exp(jnp.log(3.0) * column) * jnp.exp(jax.random.uniform(second, (D,), jnp.float32, -0.35, 0.35))
    base = jax.random.normal(first, (TOKENS, D), jnp.float32)
    return (base * column_scale[None, :]).astype(jnp.bfloat16)


def draw_q_gain(key, part):
    spread = jax.random.uniform(jax.random.fold_in(key, 21), (Q_LATENT,), jnp.float32, -1.0, 1.0)
    return (2.0 * (1.0 + 0.18 * spread)).astype(jnp.bfloat16)


def shard_levels(rng, extent, shards, low, high):
    def one(axis_at, parts):
        draws = jax.random.uniform(jax.random.fold_in(jax.random.fold_in(rng, 6), axis_at), (parts,), jnp.float32, low / len(shards), high / len(shards))
        return jnp.repeat(jnp.exp(draws), extent[axis_at] // parts).reshape((-1,) + (1,) * (len(extent) - axis_at - 1))

    loudness = one(*shards[0])
    for cut in shards[1:]:
        loudness = loudness * one(*cut)
    return loudness


def normal_values(own_key, shape, scale, bound, shards=(), held_as=jnp.bfloat16):
    drawn = jax.random.normal(own_key, shape, jnp.float32) * scale
    if len(shards) > 0:
        drawn = shard_levels(own_key, shape, shards, -0.22, 0.18) * drawn
    return jnp.clip(drawn, min=-bound, max=bound).astype(held_as)


def setup_inputs(seed: int = 0, part: int = 0) -> dict:
    keys = jax.random.split(jax.random.key(seed), 18)
    own_keys = jax.random.split(jax.random.fold_in(keys[17], part), 18)
    tokens = draw_tokens(jax.random.fold_in(jax.random.fold_in(keys[17], part), 71), part)
    mix_gain = jnp.clip(1.0 + 0.18 * jax.random.normal(keys[1], (D,), jnp.float32), 0.099609375, 1.8984375).astype(jnp.bfloat16)
    w_conv_value = normal_values(keys[2], (D, CONV_WIDTH), D ** -0.5, 0.125, ((0, 64), (1, 4)))
    w_conv_outer = normal_values(keys[3], (D, CONV_WIDTH), D ** -0.5, 0.125, ((0, 64), (1, 4)))
    w_conv_inner = normal_values(keys[4], (D, CONV_WIDTH), D ** -0.5, 0.125, ((0, 64), (1, 4)))
    conv_kernel = normal_values(keys[5], (TAPS, CONV_WIDTH), TAPS ** -0.5, 3.5, ((1, 4),))
    w_q_down = normal_values(keys[6], (D, Q_LATENT), D ** -0.5, 0.125, ((1, 4),))
    w_kv_down = normal_values(keys[7], (D, KV_LATENT), D ** -0.5, 0.125, ((1, 4),))
    w_rope_key = normal_values(keys[8], (D, ROPE), D ** -0.5, 0.125)
    q_gain = draw_q_gain(jax.random.fold_in(keys[17], 71), part)
    kv_gain = jnp.clip(1.0 + 0.18 * jax.random.normal(keys[10], (KV_LATENT,), jnp.float32), 0.099609375, 1.8984375).astype(jnp.bfloat16)
    w_q_nope = normal_values(keys[11], (Q_LATENT, MLA_HEADS * NOPE), Q_LATENT ** -0.5, 0.25, ((1, 4),))
    w_q_rope = normal_values(keys[12], (Q_LATENT, MLA_HEADS * ROPE), Q_LATENT ** -0.5, 0.25, ((1, 4),))
    w_k_nope = normal_values(keys[13], (KV_LATENT, MLA_HEADS * NOPE), KV_LATENT ** -0.5, 0.375, ((1, 4),))
    w_value = normal_values(keys[14], (KV_LATENT, MLA_HEADS * VALUE), KV_LATENT ** -0.5, 0.375, ((1, 4),))
    w_out_conv = normal_values(keys[15], (CONV_WIDTH, D), CONV_WIDTH ** -0.5, 0.1875, ((0, 4),))
    w_out_attn = normal_values(keys[16], (MLA_HEADS * VALUE, D), (max(1, MLA_HEADS * VALUE // 64)) ** -0.5, 1.5, ((0, 4),))
    return dict(tokens=tokens, mix_gain=mix_gain, w_conv_value=w_conv_value, w_conv_outer=w_conv_outer, w_conv_inner=w_conv_inner, conv_kernel=conv_kernel, w_q_down=w_q_down, w_kv_down=w_kv_down, w_rope_key=w_rope_key, q_gain=q_gain, kv_gain=kv_gain, w_q_nope=w_q_nope, w_q_rope=w_q_rope, w_k_nope=w_k_nope, w_value=w_value, w_out_conv=w_out_conv, w_out_attn=w_out_attn)


EPS = 1e-06
THETA = 10000.0

def rms_scale(values):
    return lax.rsqrt(lax.optimization_barrier(jnp.mean(values * values, axis=-1, keepdims=True)) + EPS)

def angles(positions, width):
    inverse = THETA ** (-jnp.arange(0, width, 2, dtype=jnp.float32) / width)
    phase = positions[:, None] * inverse[None, :]
    phase = jnp.concatenate([phase, phase], axis=-1)
    return (jnp.cos(phase), jnp.sin(phase))

def turned(values, cosine, sine):
    half = values.shape[-1] // 2
    first = values[..., :half]
    second = values[..., half:]
    return values * cosine + jnp.concatenate([-second, first], axis=-1) * sine

def reference(tokens, mix_gain, w_conv_value, w_conv_outer, w_conv_inner, conv_kernel, w_q_down, w_kv_down, w_rope_key, q_gain, kv_gain, w_q_nope, w_q_rope, w_k_nope, w_value, w_out_conv, w_out_attn):
    f32 = jnp.float32
    bf16 = jnp.bfloat16
    inputs = tokens.astype(f32)
    row_scale = rms_scale(inputs)
    scaled = (inputs * mix_gain.astype(f32)).astype(bf16)

    def project(weight):
        return (row_scale * jnp.dot(scaled, weight, preferred_element_type=f32)).astype(bf16)
    conv_value = project(w_conv_value)
    conv_outer = project(w_conv_outer)
    conv_inner = project(w_conv_inner)
    q_latent = project(w_q_down)
    kv_latent = project(w_kv_down)
    rope_raw = project(w_rope_key)
    gated = (conv_inner.astype(f32) * conv_value.astype(f32)).astype(bf16)
    padded = jnp.pad(gated.astype(f32), ((1, 1), (0, 0)))
    kernel = conv_kernel.astype(f32)
    conv_out = padded[:-2] * kernel[0] + padded[1:-1] * kernel[1] + padded[2:] * kernel[2]
    y_conv = (conv_outer.astype(f32) * conv_out).astype(bf16)
    q_float = q_latent.astype(f32)
    q_normed = (q_float * rms_scale(q_float) * q_gain.astype(f32)).astype(bf16)
    kv_float = kv_latent.astype(f32)
    kv_normed = (kv_float * rms_scale(kv_float) * kv_gain.astype(f32)).astype(bf16)
    count = tokens.shape[0]
    heads = w_q_nope.shape[1] // NOPE
    positions = jnp.arange(count, dtype=f32)
    cosine, sine = angles(positions, ROPE)
    q_nope = jnp.dot(q_normed, w_q_nope, preferred_element_type=f32).astype(bf16).reshape(count, heads, NOPE)
    q_rope_raw = jnp.dot(q_normed, w_q_rope, preferred_element_type=f32).reshape(count, heads, ROPE)
    q_rope = turned(q_rope_raw, cosine[:, None, :], sine[:, None, :]).astype(bf16)
    k_nope = jnp.dot(kv_normed, w_k_nope, preferred_element_type=f32).astype(bf16).reshape(count, heads, NOPE)
    values = jnp.dot(kv_normed, w_value, preferred_element_type=f32).astype(bf16).reshape(count, heads, VALUE)
    k_rope = turned(rope_raw.astype(f32), cosine, sine).astype(bf16)
    factor = (NOPE + ROPE) ** (-0.5)
    block = 128 if count % 128 == 0 else count
    keys_f = k_nope.astype(f32)
    rope_f = k_rope.astype(f32)
    values_f = values.astype(f32)

    def attend(pieces):
        query_nope, query_rope = pieces
        scores = jnp.einsum('qhd,khd->qhk', query_nope.astype(f32), keys_f)
        scores = scores + jnp.einsum('qhr,kr->qhk', query_rope.astype(f32), rope_f)
        scores = scores * factor
        peak = lax.optimization_barrier(jnp.max(scores, axis=-1, keepdims=True))
        weights = jnp.exp(scores - peak)
        total = lax.optimization_barrier(jnp.sum(weights, axis=-1))
        summed = jnp.einsum('qhk,khd->qhd', weights.astype(bf16).astype(f32), values_f)
        return (summed / total[..., None]).astype(bf16)
    blocks = count // block
    result = lax.map(attend, (q_nope.reshape(blocks, block, heads, NOPE), q_rope.reshape(blocks, block, heads, ROPE)))
    y_attn = result.reshape(count, heads * VALUE)
    conv_share = y_conv.shape[1] // N_TP
    attn_share = y_attn.shape[1] // N_TP
    summed = jnp.zeros((count, w_out_conv.shape[1]), f32)
    for index in range(N_TP):
        conv_rows = slice(index * conv_share, (index + 1) * conv_share)
        attn_rows = slice(index * attn_share, (index + 1) * attn_share)
        partial_sum = jnp.dot(y_conv[:, conv_rows], w_out_conv[conv_rows], preferred_element_type=f32)
        partial_sum = partial_sum + jnp.dot(y_attn[:, attn_rows], w_out_attn[attn_rows], preferred_element_type=f32)
        summed = summed + lax.optimization_barrier(partial_sum.astype(bf16)).astype(f32)
    return summed.astype(bf16)
```

```python
import functools
import math

import jax
import jax.numpy as jnp
from jax import lax
from jax.experimental import pallas as pl
from jax.experimental.pallas import tpu as pltpu
from jax.sharding import PartitionSpec as P

NOPE = 64
ROPE = 32
VALUE = 64
EPS = 1e-06
THETA = 10000.0
LOG2E = 1.4426950408889634
MESH = pl.DeviceIdType.MESH
F32 = jnp.float32
BF16 = jnp.bfloat16
W_AHEAD = 3


def dot_f32(a, b, contract=((1,), (0,))):
    return lax.dot_general(a, b, (contract, ((), ())), preferred_element_type=F32)


def kernel(
    SP, X,
    tokens, mix_gain, wv, wo, wi, conv_kernel, wqd, wkvd, wrk, q_gain, kv_gain,
    wqn, wqr, wkn, wval, woc, woa,
    out,
    wbuf, tok, scaled, wqd_v, wkvd_v, wrk_v, wd, wqn_v, wqr_v, wkn_v, wval_v, wval_t, wout,
    qbuf, qmine, qpart, qz, kvbuf, rope_scr, cs_scr, qg_col, kvg_col, rs_scr,
    o_acc, m_acc, l_acc, o_send, o_recv, gated, halo, yconv, rs_send, rs_recv,
    loc, tk_s, tk_r, q_s, q_r, qp_s, qp_r, kz_s, kz_r, kx_s, kx_r, wz_s, wz_r, wp_s, wp_r,
    o_s, o_r, h_s, h_r, r_s, r_r,
):
    Z = SP // 2
    HALF = Z // 2
    T = tokens.shape[0]
    DX = tokens.shape[1]
    D = DX * X
    H = wqn.shape[1] // NOPE
    sp = lax.axis_index("sp")
    x = lax.axis_index("tp")
    z = lax.div(sp, 2)
    c = lax.rem(sp, 2)
    up = lax.rem(z + 1, Z)
    dn = lax.rem(z + Z - 1, Z)
    xr = lax.rem(x + 1, X)
    xl = lax.rem(x + X - 1, X)
    xo = lax.rem(x + 2, X)
    to_up = {"sp": up * 2 + c}
    to_dn = {"sp": dn * 2 + c}
    partner = {"sp": z * 2 + 1 - c}
    to_xr, to_xl, to_xo = {"tp": xr}, {"tp": xl}, {"tp": xo}
    prev_sp = lax.rem(sp + SP - 1, SP)
    next_sp = lax.rem(sp + 1, SP)
    other_chip = {"sp": jnp.where(c == 0, prev_sp, next_sp)}

    def remote(src, dst, ssem, rsem, dev):
        return pltpu.make_async_remote_copy(
            src_ref=src, dst_ref=dst, send_sem=ssem, recv_sem=rsem, device_id=dev, device_id_type=MESH
        )

    local = []
    def bring(src, dst):
        cp = pltpu.make_async_copy(src, dst, loc.at[len(local)])
        local.append(cp)
        cp.start()
        return cp

    conv_cp = [bring(w, wbuf.at[i, z, c]) for i, w in enumerate((wv, wo, wi))]
    tok_cp = bring(tokens, tok.at[x])
    down_cp = [bring(wqd, wqd_v), bring(wkvd, wkvd_v), bring(wrk, wrk_v)]
    up_cp = [bring(wqn, wqn_v), bring(wqr, wqr_v), bring(wkn, wkn_v), bring(wval, wval_v)]
    NC = woc.shape[0]
    out_cp = [bring(woc, wout.at[pl.ds(0, NC)]), bring(woa, wout.at[pl.ds(NC, woa.shape[0])])]

    barrier = pltpu.get_barrier_semaphore()
    for dev in (to_up, to_dn, partner, to_xr, to_xl, to_xo, other_chip):
        pl.semaphore_signal(barrier, inc=1, device_id=dev, device_id_type=MESH)
    pl.semaphore_wait(barrier, 7)

    h = T // 2
    lo, hi = pl.ds(0, h), pl.ds(h, h)

    def tok_copy(k, piece, rows, dev, first):
        src = tokens.at[rows] if first else tok.at[piece, rows]
        return remote(src, tok.at[piece, rows], tk_s.at[k], tk_r.at[k], dev)

    tok_sends = [
        tok_copy(0, x, lo, to_xr, True), tok_copy(2, x, hi, to_xl, True),
        tok_copy(1, x, hi, to_xr, True), tok_copy(3, x, lo, to_xl, True),
    ]
    for cp in tok_sends:
        cp.start()

    def w_z(slot, d, way, dev):
        return remote(wbuf.at[:, slot, c], wbuf.at[:, slot, c], wz_s.at[way, d], wz_r.at[slot], dev)

    def w_p(slot, core):
        return remote(wbuf.at[:, slot, core], wbuf.at[:, slot, core], wp_s.at[slot], wp_r.at[slot], partner)

    for cp in conv_cp:
        cp.wait()
    w_z(z, 0, 0, to_up).start()
    w_z(z, 0, 1, to_dn).start()
    w_p(z, c).start()

    def when(cond, fn):
        if isinstance(cond, bool):
            if cond:
                fn()
        else:
            pl.when(cond)(fn)

    def w_step(k):
        def go_up():
            slot = lax.rem(z - k + Z, Z)
            w_z(slot, k, 0, to_up).wait_recv()
            when(k < HALF, lambda: w_z(slot, k, 0, to_up).start())
            w_p(slot, c).start()

        def go_dn():
            slot = lax.rem(z + k, Z)
            w_z(slot, k, 1, to_dn).wait_recv()
            when(k < HALF - 1, lambda: w_z(slot, k, 1, to_dn).start())
            w_p(slot, c).start()

        when(k <= HALF, go_up)
        when(k <= HALF - 1, go_dn)

    for cp in down_cp:
        cp.wait()
    wd[:, : wqd.shape[1]] = wqd_v[...]
    nk, nr = wkvd.shape[1], wrk.shape[1]
    wd[:, wqd.shape[1] :] = jnp.concatenate(
        [wkvd_v[...], wrk_v[...], jnp.zeros((D, 128 - nk - nr), BF16)], axis=1
    )
    rows16 = lax.broadcasted_iota(jnp.int32, (ROPE, T), 0)
    freq = jnp.where(rows16 >= ROPE // 2, rows16 - ROPE // 2, rows16).astype(F32) * 2.0
    inverse = jnp.exp(freq * (-math.log(THETA) / ROPE))
    phase = (sp * T + lax.broadcasted_iota(jnp.int32, (ROPE, T), 1)).astype(F32) * inverse
    cs_scr[0] = jnp.cos(phase)
    cs_scr[1] = jnp.sin(phase)
    qg_col[...] = jnp.transpose(jnp.broadcast_to(q_gain[...].astype(F32), (128, q_gain.shape[1])))
    kvg_col[...] = jnp.transpose(jnp.broadcast_to(kv_gain[...].astype(F32), (128, kv_gain.shape[1])))
    qz[...] = jnp.zeros(qz.shape, BF16)
    o_acc[...] = jnp.zeros(o_acc.shape, F32)
    m_acc[...] = jnp.full(m_acc.shape, -jnp.inf, F32)
    l_acc[...] = jnp.zeros(l_acc.shape, F32)
    for cp in up_cp:
        cp.wait()
    wval_t[...] = jnp.transpose(wval_v[...].astype(F32)).astype(BF16)

    tok_copy(0, xl, lo, to_xr, False).wait_recv()
    tok_copy(4, xl, lo, to_xr, False).start()
    tok_copy(2, xr, hi, to_xl, False).wait_recv()
    tok_copy(5, xr, hi, to_xl, False).start()
    tok_copy(1, xl, hi, to_xr, False).wait_recv()
    tok_copy(3, xr, lo, to_xl, False).wait_recv()
    w_step(1)
    tok_copy(4, xo, lo, to_xr, False).wait_recv()
    tok_copy(5, xo, hi, to_xl, False).wait_recv()
    tok_cp.wait()

    down = jnp.zeros((T, wd.shape[1]), F32)
    squares = jnp.zeros((T, 1), F32)
    for j in range(X):
        t = tok[j].astype(F32)
        s = (t * mix_gain[:, j * DX : (j + 1) * DX].astype(F32)).astype(BF16)
        scaled[:, j * DX : (j + 1) * DX] = s
        squares += jnp.sum(t * t, axis=1, keepdims=True)
        down += dot_f32(s, wd[j * DX : (j + 1) * DX, :])
    row_scale = lax.rsqrt(squares / D + EPS)
    rs_scr[...] = jnp.broadcast_to(row_scale, rs_scr.shape)
    down_t = jnp.transpose(down * row_scale)
    nq = wqd.shape[1]
    kv_rows = pl.ds(0, nk)
    kvbuf[z, x, kv_rows, :] = down_t[nq : nq + nk].astype(BF16)

    def turned(v, cosine, sine):
        half = ROPE // 2
        return v * cosine + jnp.concatenate([-v[half:], v[:half]], axis=0) * sine

    raw = down_t[nq + nk : nq + nk + nr].astype(BF16).astype(F32)
    rope_scr[...] = turned(raw, cs_scr[0], cs_scr[1])
    RX = ROPE // X
    mine = rope_scr[pl.ds(pl.multiple_of(x * RX, RX), RX), :]
    kvbuf[z, x, pl.ds(nk, 2 * RX), :] = jnp.concatenate([mine, jnp.zeros((RX, T), F32)], axis=0).astype(BF16)

    def k_z(slot, d, way, dev):
        return remote(kvbuf.at[slot, x], kvbuf.at[slot, x], kz_s.at[way, d], kz_r.at[slot], dev)

    def k_x(slot, piece, kind, dev):
        return remote(kvbuf.at[slot, piece], kvbuf.at[slot, piece], kx_s.at[slot, kind], kx_r.at[slot, kind], dev)

    k_z(z, 0, 0, to_up).start()
    k_z(z, 0, 1, to_dn).start()
    k_x(z, x, 0, to_xr).start()
    k_x(z, x, 1, to_xl).start()

    qbuf[x] = down_t[:nq].astype(BF16)

    def q_copy(kind, piece, dev):
        return remote(qbuf.at[piece], qbuf.at[piece], q_s.at[kind], q_r.at[kind], dev)

    q_sends = [q_copy(2, x, to_xo), q_copy(0, x, to_xr), q_copy(1, x, to_xl)]
    for cp in q_sends:
        cp.start()
    for k in range(2, W_AHEAD + 1):
        if k <= HALF:
            w_step(k)

    factor = (NOPE + ROPE) ** (-0.5) * LOG2E
    q_exchange = remote(qmine, qpart, qp_s.at[0], qp_r.at[0], partner)

    def make_q():
        q_copy(0, xl, to_xr).wait_recv()
        q_copy(1, xr, to_xl).wait_recv()
        q_copy(2, xo, to_xo).wait_recv()
        qf = qbuf[...].reshape(X * nq, T).astype(F32)
        scale = lax.rsqrt(jnp.mean(qf * qf, axis=0, keepdims=True) + EPS)
        qn = (qf * scale * qg_col[...]).astype(BF16)
        nope = dot_f32(wqn_v[...], qn, ((0,), (0,))) * factor
        qmine[: H * NOPE, :] = nope.astype(BF16)
        rope = dot_f32(wqr_v[...], qn, ((0,), (0,)))
        for i in range(H):
            r = turned(rope[i * ROPE : (i + 1) * ROPE], cs_scr[0], cs_scr[1]) * factor
            qmine[H * NOPE + i * ROPE : H * NOPE + (i + 1) * ROPE, :] = r.astype(BF16)
        q_exchange.start()

    def place_q():
        q_exchange.wait_recv()
        for i in range(H):
            p, e = divmod(i, 2)
            for src, at in ((qmine, 0), (qpart, T)):
                cols = slice(e * 2 * T + at, e * 2 * T + at + T)
                qz[p, e * NOPE : (e + 1) * NOPE, cols] = src[i * NOPE : (i + 1) * NOPE, :]
                qz[p, 2 * NOPE : 2 * NOPE + ROPE, cols] = src[H * NOPE + i * ROPE : H * NOPE + (i + 1) * ROPE, :]

    def keys(slot):
        lat = kvbuf[slot, :, :nk, :].reshape(X * nk, T).astype(F32)
        rope = kvbuf[slot, :, nk : nk + 2 * RX, :].astype(F32)[:, :RX].reshape(ROPE, T)
        return lat, rope

    def chunk(slot_a, slot_b):
        la, ra = keys(slot_a)
        lb, rb = keys(slot_b)
        lat = jnp.concatenate([la, lb], axis=1)
        scale = lax.rsqrt(jnp.mean(lat * lat, axis=0, keepdims=True) + EPS)
        gain = kvg_col[...]
        n = (lat * scale * jnp.concatenate([gain, gain], axis=1)).astype(BF16)
        kn = dot_f32(n, wkn_v[...], ((0,), (0,))).astype(BF16)
        rope = jnp.concatenate([ra, rb], axis=1)
        kr = jnp.transpose(jnp.concatenate([rope, jnp.zeros((128 - ROPE, 2 * T), F32)], axis=0)).astype(BF16)
        vt = dot_f32(wval_t[...], n).astype(BF16)
        for p in range(H // 2):
            kp = jnp.concatenate([kn[:, p * 128 : (p + 1) * 128], kr], axis=1)
            s = dot_f32(kp, qz[p])
            old = m_acc[p]
            new = jnp.maximum(old, jnp.max(s, axis=0, keepdims=True))
            m_acc[p] = new
            fade = jnp.exp2(old - new)
            w = jnp.exp2(s - new)
            l_acc[p] = l_acc[p] * fade + jnp.sum(w, axis=0, keepdims=True)
            wb = w.astype(BF16)
            for e in range(2):
                i = 2 * p + e
                cols = slice(e * 2 * T, (e + 1) * 2 * T)
                o_acc[i] = o_acc[i] * fade[:, cols] + dot_f32(vt[i * VALUE : (i + 1) * VALUE], wb[:, cols])

    def halo_copy(k, dev):
        rows = pl.ds(0, 8) if k == 1 else pl.ds(T - 8, 8)
        return remote(gated.at[rows], halo.at[k], h_s.at[k], h_r.at[k], dev)

    to_next, to_prev = {"sp": next_sp}, {"sp": prev_sp}

    def conv_gates():
        def got(s, _):
            w_p(s, 1 - c).wait_recv()
            return 0
        lax.fori_loop(0, Z, got, 0)
        def project(i):
            w = wbuf[i].reshape(D, wbuf.shape[-1])
            return (dot_f32(scaled[...], w) * rs_scr[:, 0:1]).astype(BF16).astype(F32)
        inner = project(2)
        value = project(0)
        gated[...] = (inner * value).astype(BF16).astype(F32)
        halo_copy(0, to_next).start()
        halo_copy(1, to_prev).start()
        yconv[...] = project(1)

    def step(d, _):
        def up_in():
            slot = lax.rem(z - d + Z, Z)
            k_z(slot, d, 0, to_up).wait_recv()
            pl.when(d < HALF)(lambda: k_z(slot, d, 0, to_up).start())
            k_x(slot, x, 0, to_xr).start()
            k_x(slot, x, 1, to_xl).start()

        def dn_in():
            slot = lax.rem(z + d, Z)
            k_z(slot, d, 1, to_dn).wait_recv()
            pl.when(d < HALF - 1)(lambda: k_z(slot, d, 1, to_dn).start())
            k_x(slot, x, 0, to_xr).start()
            k_x(slot, x, 1, to_xl).start()

        pl.when(d <= HALF)(up_in)
        pl.when(d <= HALF - 1)(dn_in)

        e = d - 1

        def relay_up():
            slot = lax.rem(z - e + Z, Z)
            k_x(slot, xl, 0, to_xr).wait_recv()
            k_x(slot, xl, 2, to_xr).start()

        def relay_dn():
            slot = lax.rem(z + e, Z)
            k_x(slot, xr, 1, to_xl).wait_recv()
            k_x(slot, xr, 2, to_xl).start()

        pl.when(e <= HALF)(relay_up)
        pl.when(jnp.logical_and(e >= 1, e <= HALF - 1))(relay_dn)

        w_step(d + W_AHEAD)

        pl.when(d == 1)(make_q)
        pl.when(d == 2)(place_q)
        pl.when(d == HALF + 1)(conv_gates)

        g = d - 2
        last = g == HALF
        slot_a = lax.rem(z - g + Z, Z)
        slot_b = jnp.where(last, z, lax.rem(z + g, Z))

        def attend():
            k_x(slot_a, xr, 1, to_xl).wait_recv()
            k_x(slot_a, xo, 2, to_xr).wait_recv()

            def up_kind():
                k_x(slot_b, xr, 1, to_xl).wait_recv()

            def dn_kind():
                k_x(slot_b, xl, 0, to_xr).wait_recv()

            pl.when(last)(up_kind)
            pl.when(jnp.logical_not(last))(dn_kind)
            k_x(slot_b, xo, 2, to_xr).wait_recv()
            chunk(slot_a, slot_b)

        pl.when(g >= 1)(attend)
        return 0

    lax.fori_loop(1, HALF + 3, step, 0)

    for i in range(H):
        p, e = divmod(i, 2)
        theirs = slice(e * 2 * T + T, (e + 1) * 2 * T)
        o_send[i * VALUE : (i + 1) * VALUE, :] = o_acc[i][:, T:]
        o_send[H * VALUE + i : H * VALUE + i + 1, :] = m_acc[p][:, theirs]
        o_send[H * VALUE + H + i : H * VALUE + H + i + 1, :] = l_acc[p][:, theirs]
    o_exchange = remote(o_send, o_recv, o_s.at[0], o_r.at[0], partner)
    o_exchange.start()

    halo_copy(0, to_next).wait_recv()
    halo_copy(1, to_prev).wait_recv()
    g = gated[...]
    row = lax.broadcasted_iota(jnp.int32, g.shape, 0)
    before = jnp.where(sp == 0, 0.0, halo[0, 7:8, :])
    after = jnp.where(sp == SP - 1, 0.0, halo[1, 0:1, :])
    g_before = jnp.where(row == 0, before, pltpu.roll(g, 1, 0))
    g_after = jnp.where(row == T - 1, after, pltpu.roll(g, T - 1, 0))
    taps = conv_kernel[...].astype(F32)
    conv = g_before * taps[0:1] + g * taps[1:2] + g_after * taps[2:3]
    y_conv = (yconv[...] * conv).astype(BF16)

    o_exchange.wait_recv()
    parts = []
    for i in range(H):
        p, e = divmod(i, 2)
        ours = slice(e * 2 * T, e * 2 * T + T)
        m1 = m_acc[p][:, ours]
        m2 = o_recv[H * VALUE + i : H * VALUE + i + 1, :]
        top = jnp.maximum(m1, m2)
        a1, a2 = jnp.exp2(m1 - top), jnp.exp2(m2 - top)
        total = a1 * l_acc[p][:, ours] + a2 * o_recv[H * VALUE + H + i : H * VALUE + H + i + 1, :]
        summed = a1 * o_acc[i][:, :T] + a2 * o_recv[i * VALUE : (i + 1) * VALUE, :]
        parts.append(summed / total)
    y_attn = jnp.transpose(jnp.concatenate(parts, axis=0)).astype(BF16)
    y = jnp.concatenate([y_conv, y_attn], axis=1)
    for cp in out_cp:
        cp.wait()
    for rel, dev in ((2, to_xo), (1, to_xr), (3, to_xl), (0, None)):
        dest = lax.rem(x + rel, X)
        cols = pl.ds(pl.multiple_of(dest * DX, DX), DX)
        rs_send[rel] = dot_f32(y, wout[:, cols]).astype(BF16)
        if dev is not None:
            remote(rs_send.at[rel], rs_recv.at[rel - 1], r_s.at[rel - 1], r_r.at[rel - 1], dev).start()
    total = rs_send[0].astype(F32)
    r_copies = [
        remote(rs_send.at[rel], rs_recv.at[rel - 1], r_s.at[rel - 1], r_r.at[rel - 1], dev)
        for rel, dev in ((1, to_xr), (3, to_xl), (2, to_xo))
    ]
    for rel, cp in zip((1, 3, 2), r_copies):
        cp.wait_recv()
        total += rs_recv[rel - 1].astype(F32)
    out[...] = total.astype(BF16)

    for cp in tok_sends + [tok_copy(4, xl, lo, to_xr, False), tok_copy(5, xr, hi, to_xl, False)]:
        cp.wait_send()
    for cp in q_sends + [q_exchange, halo_copy(0, to_next), halo_copy(1, to_prev), o_exchange] + r_copies:
        cp.wait_send()

    def sent(d, _):
        k_z(z, d, 0, to_up).wait_send()
        w_z(z, d, 0, to_up).wait_send()

        def back():
            k_z(z, d, 1, to_dn).wait_send()
            w_z(z, d, 1, to_dn).wait_send()

        pl.when(d < HALF - 1)(back)
        return 0

    lax.fori_loop(0, HALF, sent, 0)

    def sent_slots(s, _):
        w_p(s, c).wait_send()
        for kind, dev in ((0, to_xr), (1, to_xl), (2, to_xr)):
            k_x(s, x, kind, dev).wait_send()
        return 0

    lax.fori_loop(0, Z, sent_slots, 0)


def solution(mesh):
    SP, X = mesh.shape["sp"], mesh.shape["tp"]

    def per_device(
        tokens, mix_gain, wv, wo, wi, conv_kernel, wqd, wkvd, wrk, q_gain, kv_gain,
        wqn, wqr, wkn, wval, woc, woa,
    ):
        T, DX = tokens.shape
        D = DX * X
        Z = SP // 2
        R, CC = wv.shape
        H = wqn.shape[1] // NOPE
        nk, nq = wkvd.shape[1], wqd.shape[1]
        RX = ROPE // X
        anyspace = pl.BlockSpec(memory_space=pl.ANY)
        vmem = pl.BlockSpec(memory_space=pltpu.VMEM)
        V = pltpu.VMEM
        DMA = pltpu.SemaphoreType.DMA
        scratch = [
            V((3, Z, 2, R, CC), BF16),
            V((X, T, DX), BF16),
            V((T, D), BF16),
            V(wqd.shape, BF16), V(wkvd.shape, BF16), V(wrk.shape, BF16),
            V((D, nq + 128), BF16),
            V(wqn.shape, BF16), V(wqr.shape, BF16), V(wkn.shape, BF16), V(wval.shape, BF16),
            V((wval.shape[1], wval.shape[0]), BF16),
            V((woc.shape[0] + woa.shape[0], woc.shape[1]), BF16),
            V((X, nq, T), BF16),
            V((H * (NOPE + ROPE), T), BF16), V((H * (NOPE + ROPE), T), BF16),
            V((H // 2, 256, 4 * T), BF16),
            V((Z, X, nk + 2 * RX, T), BF16),
            V((ROPE, T), F32), V((2, ROPE, T), F32),
            V((nq * X, 128), F32), V((nk * X, 128), F32),
            V((T, 128), F32),
            V((H, VALUE, 2 * T), F32), V((H // 2, 1, 4 * T), F32), V((H // 2, 1, 4 * T), F32),
            V((H * VALUE + 2 * H, T), F32), V((H * VALUE + 2 * H, T), F32),
            V((T, CC), F32), V((2, 8, CC), F32), V((T, CC), F32),
            V((X, T, DX), BF16), V((X - 1, T, DX), BF16),
            DMA((13,)),
            DMA((6,)), DMA((6,)),
            DMA((3,)), DMA((3,)), DMA((1,)), DMA((1,)),
            DMA((2, Z // 2)), DMA((Z,)), DMA((Z, 3)), DMA((Z, 3)),
            DMA((2, Z // 2)), DMA((Z,)), DMA((Z,)), DMA((Z,)),
            DMA((1,)), DMA((1,)), DMA((2,)), DMA((2,)), DMA((3,)), DMA((3,)),
        ]
        return pl.pallas_call(
            functools.partial(kernel, SP, X),
            out_shape=jax.ShapeDtypeStruct((T, DX), BF16),
            in_specs=[anyspace, vmem, anyspace, anyspace, anyspace, vmem, anyspace, anyspace, anyspace,
                      vmem, vmem] + [anyspace] * 6,
            out_specs=vmem,
            scratch_shapes=scratch,
            compiler_params=pltpu.CompilerParams(
                collective_id=0, has_side_effects=True, vmem_limit_bytes=56 * 1024 * 1024
            ),
        )(
            tokens, mix_gain.reshape(1, -1), wv, wo, wi, conv_kernel, wqd, wkvd, wrk,
            q_gain.reshape(1, -1), kv_gain.reshape(1, -1), wqn, wqr, wkn, wval, woc, woa,
        )

    placed = (
        P(("grp", "sp"), "tp"),
        P(),
        P("sp", "tp"),
        P("sp", "tp"),
        P("sp", "tp"),
        P(None, "tp"),
        P(None, "tp"),
        P(None, "tp"),
        P(),
        P(),
        P(),
        P(None, "tp"),
        P(None, "tp"),
        P(None, "tp"),
        P(None, "tp"),
        P("tp", None),
        P("tp", None),
    )
    return jax.shard_map(
        per_device, mesh=mesh, in_specs=placed, out_specs=P(("grp", "sp"), "tp"), check_vma=False
    )
```

```python
import functools
import math

import jax
import jax.numpy as jnp
from jax import lax
from jax.experimental import pallas as pl
from jax.experimental.pallas import tpu as pltpu
from jax.sharding import PartitionSpec as P

NOPE = 64
ROPE = 32
VALUE = 64
EPS = 1e-06
THETA = 10000.0
LOG2E = 1.4426950408889634
MESH = pl.DeviceIdType.MESH
F32 = jnp.float32
BF16 = jnp.bfloat16
STRIDE = 3
W_FIRST = 3
W_EACH = 2


def dot_f32(a, b, contract=((1,), (0,))):
    return lax.dot_general(a, b, (contract, ((), ())), preferred_element_type=F32)


def kernel(
    SP, X,
    tokens, mix_gain, wv, wo, wi, conv_kernel, wqd, wkvd, wrk, q_gain, kv_gain,
    wqn, wqr, wkn, wval, woc, woa,
    out,
    wbuf, tok, scaled, wqd_v, wd_t, wqn_v, wqr_v, wkn_v, wval_v, wval_t, wout,
    qbuf, qmine, qpart, qz, kvbuf, rope_scr, cs_scr, qg_col, kvg_col, rs_scr,
    o_acc, m_acc, l_acc, o_send, o_recv, gated, halo, yconv, rs_send, rs_recv,
    loc, tk_s, tk_r, q_s, q_r, qp_s, qp_r, kf_s, kn_s, kz_r, kx_s, kx_r, wz_s, wz_r, wp_s, wp_r, wq_s, wq_r,
    o_s, o_r, h_s, h_r, r_s, r_r,
):
    Z = SP // 2
    HALF = Z // 2
    K = (HALF - 1) // STRIDE
    assert HALF == STRIDE * K + 1
    T = tokens.shape[0]
    DX = tokens.shape[1]
    D = DX * X
    H = wqn.shape[1] // NOPE
    sp = lax.axis_index("sp")
    x = lax.axis_index("tp")
    z = lax.div(sp, 2)
    c = lax.rem(sp, 2)
    def core_at(step):
        return {"sp": lax.rem(z + step + Z, Z) * 2 + c}

    xr = lax.rem(x + 1, X)
    xl = lax.rem(x + X - 1, X)
    xo = lax.rem(x + 2, X)
    to_up, to_dn = core_at(1), core_at(-1)
    far_up, far_dn = core_at(STRIDE), core_at(-STRIDE)
    partner = {"sp": z * 2 + 1 - c}
    to_xr, to_xl, to_xo = {"tp": xr}, {"tp": xl}, {"tp": xo}
    prev_sp = lax.rem(sp + SP - 1, SP)
    next_sp = lax.rem(sp + 1, SP)
    other_chip = {"sp": jnp.where(c == 0, prev_sp, next_sp)}

    def remote(src, dst, ssem, rsem, dev):
        return pltpu.make_async_remote_copy(
            src_ref=src, dst_ref=dst, send_sem=ssem, recv_sem=rsem, device_id=dev, device_id_type=MESH
        )

    local = []
    def bring(src, dst):
        cp = pltpu.make_async_copy(src, dst, loc.at[len(local)])
        local.append(cp)
        cp.start()
        return cp

    conv_cp = [bring(w, wbuf.at[i, z, c]) for i, w in enumerate((wv, wo, wi))]
    tok_cp = bring(tokens, tok.at[x])
    nk, nr = wkvd.shape[0], wrk.shape[0]
    down_cp = [bring(wqd, wqd_v), bring(wkvd, wd_t.at[pl.ds(0, nk)]), bring(wrk, wd_t.at[pl.ds(nk, nr)])]
    up_cp = [bring(wqn, wqn_v), bring(wqr, wqr_v), bring(wkn, wkn_v), bring(wval, wval_v)]
    NC = woc.shape[0]
    out_cp = [bring(woc, wout.at[pl.ds(0, NC)]), bring(woa, wout.at[pl.ds(NC, woa.shape[0])])]

    barrier = pltpu.get_barrier_semaphore()
    for dev in (to_up, to_dn, far_up, far_dn, partner, to_xr, to_xl, to_xo, other_chip):
        pl.semaphore_signal(barrier, inc=1, device_id=dev, device_id_type=MESH)
    pl.semaphore_wait(barrier, 9)

    h = T // 2
    lo, hi = pl.ds(0, h), pl.ds(h, h)

    def tok_copy(k, piece, rows, dev, first):
        src = tokens.at[rows] if first else tok.at[piece, rows]
        return remote(src, tok.at[piece, rows], tk_s.at[k], tk_r.at[k], dev)

    tok_sends = [
        tok_copy(0, x, lo, to_xr, True), tok_copy(2, x, hi, to_xl, True),
        tok_copy(1, x, hi, to_xr, True), tok_copy(3, x, lo, to_xl, True),
    ]
    for cp in tok_sends:
        cp.start()

    def w_z(slot, d, way, core, dev):
        piece = wbuf.at[:, slot, core]
        return remote(piece, piece, wz_s.at[way, d, core], wz_r.at[slot, core], dev)

    def w_p(slot):
        return remote(wbuf.at[:, slot], wbuf.at[:, slot], wp_s.at[slot], wp_r.at[slot], partner)

    def w_own(core):
        return remote(wbuf.at[:, z, core], wbuf.at[:, z, core], wq_s.at[0], wq_r.at[0], partner)

    for cp in conv_cp:
        cp.wait()
    w_own(c).start()

    def w_begin(core):
        w_z(z, 0, 0, core, to_up).start()
        w_z(z, 0, 1, core, to_dn).start()

    pl.when(c == 1)(lambda: w_begin(1))

    def w_in(k, way):
        slot = lax.rem(z - k + Z, Z) if way == 0 else lax.rem(z + k, Z)
        dev = to_up if way == 0 else to_dn
        end = HALF if way == 0 else HALF - 1
        for core in (1, 0):
            w_z(slot, k, way, core, dev).wait_recv()
            pl.when(k < end)(lambda core=core: w_z(slot, k, way, core, dev).start())
        w_p(slot).start()

    def w_step(k):
        pl.when(jnp.logical_and(c == 1, k <= HALF))(lambda: w_in(k, 0))
        pl.when(jnp.logical_and(c == 1, k <= HALF - 1))(lambda: w_in(k, 1))

    def w_steps(first, count):
        def one(i, _):
            w_step(first + i)
            return 0
        lax.fori_loop(0, count, one, 0)

    wd_t[nk + nr :, :] = jnp.zeros((wd_t.shape[0] - nk - nr, D), BF16)
    rows16 = lax.broadcasted_iota(jnp.int32, (ROPE, T), 0)
    freq = jnp.where(rows16 >= ROPE // 2, rows16 - ROPE // 2, rows16).astype(F32) * 2.0
    inverse = jnp.exp(freq * (-math.log(THETA) / ROPE))
    phase = (sp * T + lax.broadcasted_iota(jnp.int32, (ROPE, T), 1)).astype(F32) * inverse
    cs_scr[0] = jnp.cos(phase)
    cs_scr[1] = jnp.sin(phase)
    qg_col[...] = jnp.transpose(jnp.broadcast_to(q_gain[...].astype(F32), (128, q_gain.shape[1])))
    kvg_col[...] = jnp.transpose(jnp.broadcast_to(kv_gain[...].astype(F32), (128, kv_gain.shape[1])))
    qz[...] = jnp.zeros(qz.shape, BF16)
    o_acc[...] = jnp.zeros(o_acc.shape, F32)
    m_acc[...] = jnp.full(m_acc.shape, -jnp.inf, F32)
    l_acc[...] = jnp.zeros(l_acc.shape, F32)
    for cp in up_cp:
        cp.wait()
    wval_t[...] = jnp.transpose(wval_v[...].astype(F32)).astype(BF16)

    w_own(1 - c).wait_recv()
    pl.when(c == 1)(lambda: w_begin(0))
    tok_copy(0, xl, lo, to_xr, False).wait_recv()
    tok_copy(4, xl, lo, to_xr, False).start()
    tok_copy(2, xr, hi, to_xl, False).wait_recv()
    tok_copy(5, xr, hi, to_xl, False).start()
    tok_copy(1, xl, hi, to_xr, False).wait_recv()
    tok_copy(3, xr, lo, to_xl, False).wait_recv()
    w_steps(1, 1)
    tok_copy(4, xo, lo, to_xr, False).wait_recv()
    tok_copy(5, xo, hi, to_xl, False).wait_recv()
    tok_cp.wait()

    for cp in down_cp:
        cp.wait()
    down_q = jnp.zeros((T, wqd.shape[1]), F32)
    down_k = jnp.zeros((T, wd_t.shape[0]), F32)
    squares = jnp.zeros((T, 1), F32)
    for j in range(X):
        t = tok[j].astype(F32)
        s = (t * mix_gain[:, j * DX : (j + 1) * DX].astype(F32)).astype(BF16)
        scaled[:, j * DX : (j + 1) * DX] = s
        squares += jnp.sum(t * t, axis=1, keepdims=True)
        down_q += dot_f32(s, wqd_v[j * DX : (j + 1) * DX, :])
        down_k += dot_f32(s, wd_t[:, j * DX : (j + 1) * DX], ((1,), (1,)))
    row_scale = lax.rsqrt(squares / D + EPS)
    rs_scr[...] = jnp.broadcast_to(row_scale, rs_scr.shape)
    down_t = jnp.transpose(jnp.concatenate([down_q, down_k], axis=1) * row_scale)
    nq = wqd.shape[1]
    kv_rows = pl.ds(0, nk)
    kvbuf[z, x, kv_rows, :] = down_t[nq : nq + nk].astype(BF16)

    def turned(v, cosine, sine):
        half = ROPE // 2
        return v * cosine + jnp.concatenate([-v[half:], v[:half]], axis=0) * sine

    raw = down_t[nq + nk : nq + nk + nr].astype(BF16).astype(F32)
    rope_scr[...] = turned(raw, cs_scr[0], cs_scr[1])
    RX = ROPE // X
    mine = rope_scr[pl.ds(pl.multiple_of(x * RX, RX), RX), :]
    kvbuf[z, x, pl.ds(nk, 2 * RX), :] = jnp.concatenate([mine, jnp.zeros((RX, T), F32)], axis=0).astype(BF16)

    def k_far(slot, j, way):
        piece = kvbuf.at[slot, x]
        return remote(piece, piece, kf_s.at[way, j], kz_r.at[slot], far_dn if way else far_up)

    def k_near(slot, way):
        piece = kvbuf.at[slot, x]
        return remote(piece, piece, kn_s.at[slot, way], kz_r.at[slot], to_dn if way else to_up)

    def k_x(slot, piece, kind, dev):
        return remote(kvbuf.at[slot, piece], kvbuf.at[slot, piece], kx_s.at[slot, kind], kx_r.at[slot, kind], dev)

    k_far(z, 0, 0).start()
    k_far(z, 0, 1).start()
    k_near(z, 0).start()
    k_near(z, 1).start()
    k_x(z, x, 0, to_xr).start()
    k_x(z, x, 1, to_xl).start()

    qbuf[x] = down_t[:nq].astype(BF16)

    def q_copy(kind, piece, dev):
        return remote(qbuf.at[piece], qbuf.at[piece], q_s.at[kind], q_r.at[kind], dev)

    q_sends = [q_copy(2, x, to_xo), q_copy(0, x, to_xr), q_copy(1, x, to_xl)]
    for cp in q_sends:
        cp.start()
    w_steps(2, W_FIRST - 1)

    factor = (NOPE + ROPE) ** (-0.5) * LOG2E
    q_exchange = remote(qmine, qpart, qp_s.at[0], qp_r.at[0], partner)

    def make_q():
        q_copy(0, xl, to_xr).wait_recv()
        q_copy(1, xr, to_xl).wait_recv()
        q_copy(2, xo, to_xo).wait_recv()
        qf = qbuf[...].reshape(X * nq, T).astype(F32)
        scale = lax.rsqrt(jnp.mean(qf * qf, axis=0, keepdims=True) + EPS)
        qn = (qf * scale * qg_col[...]).astype(BF16)
        nope = dot_f32(wqn_v[...], qn, ((0,), (0,))) * factor
        qmine[: H * NOPE, :] = nope.astype(BF16)
        rope = dot_f32(wqr_v[...], qn, ((0,), (0,)))
        for i in range(H):
            r = turned(rope[i * ROPE : (i + 1) * ROPE], cs_scr[0], cs_scr[1]) * factor
            qmine[H * NOPE + i * ROPE : H * NOPE + (i + 1) * ROPE, :] = r.astype(BF16)
        q_exchange.start()

    def place_q():
        q_exchange.wait_recv()
        for i in range(H):
            p, e = divmod(i, 2)
            for src, at in ((qmine, 0), (qpart, T)):
                cols = slice(e * 2 * T + at, e * 2 * T + at + T)
                qz[p, e * NOPE : (e + 1) * NOPE, cols] = src[i * NOPE : (i + 1) * NOPE, :]
                qz[p, 2 * NOPE : 2 * NOPE + ROPE, cols] = src[H * NOPE + i * ROPE : H * NOPE + (i + 1) * ROPE, :]

    def keys(slot):
        lat = kvbuf[slot, :, :nk, :].reshape(X * nk, T).astype(F32)
        rope = kvbuf[slot, :, nk : nk + 2 * RX, :].astype(F32)[:, :RX].reshape(ROPE, T)
        return lat, rope

    def chunk(slot_a, slot_b):
        la, ra = keys(slot_a)
        lb, rb = keys(slot_b)
        lat = jnp.concatenate([la, lb], axis=1)
        scale = lax.rsqrt(jnp.mean(lat * lat, axis=0, keepdims=True) + EPS)
        gain = kvg_col[...]
        n = (lat * scale * jnp.concatenate([gain, gain], axis=1)).astype(BF16)
        kn = dot_f32(n, wkn_v[...], ((0,), (0,))).astype(BF16)
        rope = jnp.concatenate([ra, rb], axis=1)
        kr = jnp.transpose(jnp.concatenate([rope, jnp.zeros((128 - ROPE, 2 * T), F32)], axis=0)).astype(BF16)
        vt = dot_f32(wval_t[...], n).astype(BF16)
        for p in range(H // 2):
            kp = jnp.concatenate([kn[:, p * 128 : (p + 1) * 128], kr], axis=1)
            s = dot_f32(kp, qz[p])
            old = m_acc[p]
            new = jnp.maximum(old, jnp.max(s, axis=0, keepdims=True))
            m_acc[p] = new
            fade = jnp.exp2(old - new)
            w = jnp.exp2(s - new)
            l_acc[p] = l_acc[p] * fade + jnp.sum(w, axis=0, keepdims=True)
            wb = w.astype(BF16)
            for e in range(2):
                i = 2 * p + e
                cols = slice(e * 2 * T, (e + 1) * 2 * T)
                o_acc[i] = o_acc[i] * fade[:, cols] + dot_f32(vt[i * VALUE : (i + 1) * VALUE], wb[:, cols])

    def halo_copy(k, dev):
        rows = pl.ds(0, 8) if k == 1 else pl.ds(T - 8, 8)
        return remote(gated.at[rows], halo.at[k], h_s.at[k], h_r.at[k], dev)

    to_next, to_prev = {"sp": next_sp}, {"sp": prev_sp}

    def conv_gates():
        def got(i, _):
            w_p(lax.rem(z + i, Z)).wait_recv()
            return 0

        def all_in():
            lax.fori_loop(1, Z, got, 0)

        pl.when(c == 0)(all_in)

        def project(i):
            w = wbuf[i].reshape(D, wbuf.shape[-1])
            return (dot_f32(scaled[...], w) * rs_scr[:, 0:1]).astype(BF16).astype(F32)
        inner = project(2)
        value = project(0)
        gated[...] = (inner * value).astype(BF16).astype(F32)
        halo_copy(0, to_next).start()
        halo_copy(1, to_prev).start()
        yconv[...] = project(1)

    def at(offset):
        return lax.rem(z + offset + 2 * Z, Z)

    def spread(slot):
        k_x(slot, x, 0, to_xr).start()
        k_x(slot, x, 1, to_xl).start()

    def stop(j, way):
        slot = at(STRIDE * j if way else -STRIDE * j)
        k_near(slot, 0).wait_recv()
        pl.when(j < K)(lambda: k_far(slot, j, way).start())
        if way == 0:
            k_near(slot, 0).start()
            k_near(slot, 1).start()
        else:
            k_near(slot, 0).start()
            pl.when(j < K)(lambda: k_near(slot, 1).start())
        spread(slot)

    def leaf(slot):
        k_near(slot, 0).wait_recv()
        spread(slot)

    def relay_up(slot):
        k_x(slot, xl, 0, to_xr).wait_recv()
        k_x(slot, xl, 2, to_xr).start()

    def relay_dn(slot):
        k_x(slot, xr, 1, to_xl).wait_recv()
        k_x(slot, xr, 2, to_xl).start()

    def leaves(j, fn_up, fn_dn):
        def inner():
            fn_up(at(-STRIDE * j + 1))
            fn_dn(at(STRIDE * j - 1))

        fn_up(at(-STRIDE * j - 1))
        pl.when(j < K)(lambda: fn_dn(at(STRIDE * j + 1)))
        pl.when(j >= 1)(inner)

    def got_up(slot):
        k_x(slot, xr, 1, to_xl).wait_recv()
        k_x(slot, xo, 2, to_xr).wait_recv()

    def got_dn(slot):
        k_x(slot, xl, 0, to_xr).wait_recv()
        k_x(slot, xo, 2, to_xl).wait_recv()

    def pair(j, r):
        off = STRIDE * j + jnp.where(r == 0, 0, jnp.where(r == 1, -1, 1))
        own = off == HALF
        slot_a = at(-off)
        slot_b = jnp.where(own, z, at(off))
        got_up(slot_a)
        pl.when(own)(lambda: got_up(slot_b))
        pl.when(jnp.logical_not(own))(lambda: got_dn(slot_b))
        chunk(slot_a, slot_b)

    def step(i, _):
        def stops_in():
            stop(i, 0)
            stop(i, 1)

        pl.when(i <= K)(stops_in)
        pl.when(i - 1 <= K)(lambda: leaves(i - 1, leaf, leaf))

        def relay_stops():
            relay_up(at(-STRIDE * (i - 1)))
            pl.when(i - 1 >= 1)(lambda: relay_dn(at(STRIDE * (i - 1))))

        pl.when(i - 1 <= K)(relay_stops)
        pl.when(jnp.logical_and(i - 2 >= 0, i - 2 <= K))(lambda: leaves(i - 2, relay_up, relay_dn))

        pl.when(i <= K + 1)(lambda: w_steps(W_FIRST + 1 + W_EACH * (i - 1), W_EACH))

        pl.when(i == 1)(make_q)
        pl.when(i == 2)(place_q)
        pl.when(i == K + 1)(w_rest)

        def one(r, _):
            j = jnp.where(r == 0, i - 2, i - 3)
            here = jnp.logical_and(j >= jnp.where(r == 2, 0, 1), j <= K)
            pl.when(here)(lambda: pair(j, r))
            return 0

        lax.fori_loop(0, 3, one, 0)
        return 0

    def w_rest():
        w_steps(W_FIRST + 1 + W_EACH * (K + 1), HALF - W_FIRST - W_EACH * (K + 1))
        conv_gates()

    lax.fori_loop(1, K + 4, step, 0)

    for i in range(H):
        p, e = divmod(i, 2)
        theirs = slice(e * 2 * T + T, (e + 1) * 2 * T)
        o_send[i * VALUE : (i + 1) * VALUE, :] = o_acc[i][:, T:]
        o_send[H * VALUE + i : H * VALUE + i + 1, :] = m_acc[p][:, theirs]
        o_send[H * VALUE + H + i : H * VALUE + H + i + 1, :] = l_acc[p][:, theirs]
    o_exchange = remote(o_send, o_recv, o_s.at[0], o_r.at[0], partner)
    o_exchange.start()

    halo_copy(0, to_next).wait_recv()
    halo_copy(1, to_prev).wait_recv()
    g = gated[...]
    row = lax.broadcasted_iota(jnp.int32, g.shape, 0)
    before = jnp.where(sp == 0, 0.0, halo[0, 7:8, :])
    after = jnp.where(sp == SP - 1, 0.0, halo[1, 0:1, :])
    g_before = jnp.where(row == 0, before, pltpu.roll(g, 1, 0))
    g_after = jnp.where(row == T - 1, after, pltpu.roll(g, T - 1, 0))
    taps = conv_kernel[...].astype(F32)
    conv = g_before * taps[0:1] + g * taps[1:2] + g_after * taps[2:3]
    y_conv = (yconv[...] * conv).astype(BF16)

    o_exchange.wait_recv()
    parts = []
    for i in range(H):
        p, e = divmod(i, 2)
        ours = slice(e * 2 * T, e * 2 * T + T)
        m1 = m_acc[p][:, ours]
        m2 = o_recv[H * VALUE + i : H * VALUE + i + 1, :]
        top = jnp.maximum(m1, m2)
        a1, a2 = jnp.exp2(m1 - top), jnp.exp2(m2 - top)
        total = a1 * l_acc[p][:, ours] + a2 * o_recv[H * VALUE + H + i : H * VALUE + H + i + 1, :]
        summed = a1 * o_acc[i][:, :T] + a2 * o_recv[i * VALUE : (i + 1) * VALUE, :]
        parts.append(summed / total)
    y_attn = jnp.transpose(jnp.concatenate(parts, axis=0)).astype(BF16)
    y = jnp.concatenate([y_conv, y_attn], axis=1)
    for cp in out_cp:
        cp.wait()
    for rel, dev in ((2, to_xo), (1, to_xr), (3, to_xl), (0, None)):
        dest = lax.rem(x + rel, X)
        cols = pl.ds(pl.multiple_of(dest * DX, DX), DX)
        rs_send[rel] = dot_f32(y, wout[:, cols]).astype(BF16)
        if dev is not None:
            remote(rs_send.at[rel], rs_recv.at[rel - 1], r_s.at[rel - 1], r_r.at[rel - 1], dev).start()
    total = rs_send[0].astype(F32)
    r_copies = [
        remote(rs_send.at[rel], rs_recv.at[rel - 1], r_s.at[rel - 1], r_r.at[rel - 1], dev)
        for rel, dev in ((1, to_xr), (3, to_xl), (2, to_xo))
    ]
    for rel, cp in zip((1, 3, 2), r_copies):
        cp.wait_recv()
        total += rs_recv[rel - 1].astype(F32)
    out[...] = total.astype(BF16)

    for cp in tok_sends + [tok_copy(4, xl, lo, to_xr, False), tok_copy(5, xr, hi, to_xl, False)]:
        cp.wait_send()
    for cp in q_sends + [q_exchange, halo_copy(0, to_next), halo_copy(1, to_prev), o_exchange] + r_copies:
        cp.wait_send()

    w_own(c).wait_send()

    def w_sent(d, _):
        for core in (0, 1):
            w_z(z, d, 0, core, to_up).wait_send()

        def back():
            for core in (0, 1):
                w_z(z, d, 1, core, to_dn).wait_send()

        pl.when(d < HALF - 1)(back)
        return 0

    def w_handed(i, _):
        w_p(lax.rem(z + i, Z)).wait_send()
        return 0

    def w_all():
        lax.fori_loop(0, HALF, w_sent, 0)
        lax.fori_loop(1, Z, w_handed, 0)

    pl.when(c == 1)(w_all)

    def k_sent(j, _):
        for way in (0, 1):
            pl.when(j < K)(lambda way=way: k_far(z, j, way).wait_send())
        k_near(at(-STRIDE * j), 0).wait_send()
        k_near(at(-STRIDE * j), 1).wait_send()

        def back():
            k_near(at(STRIDE * j), 0).wait_send()
            pl.when(j < K)(lambda: k_near(at(STRIDE * j), 1).wait_send())

        pl.when(j >= 1)(back)
        return 0

    lax.fori_loop(0, K + 1, k_sent, 0)

    def sent_slots(s, _):
        for kind, dev in ((0, to_xr), (1, to_xl), (2, to_xr)):
            k_x(s, x, kind, dev).wait_send()
        return 0

    lax.fori_loop(0, Z, sent_slots, 0)


def solution(mesh):
    SP, X = mesh.shape["sp"], mesh.shape["tp"]

    def per_device(
        tokens, mix_gain, wv, wo, wi, conv_kernel, wqd, wkvd, wrk, q_gain, kv_gain,
        wqn, wqr, wkn, wval, woc, woa,
    ):
        T, DX = tokens.shape
        D = DX * X
        Z = SP // 2
        R, CC = wv.shape
        H = wqn.shape[1] // NOPE
        nk, nq = wkvd.shape[1], wqd.shape[1]
        K = (Z // 2 - 1) // STRIDE
        RX = ROPE // X
        anyspace = pl.BlockSpec(memory_space=pl.ANY)
        vmem = pl.BlockSpec(memory_space=pltpu.VMEM)
        V = pltpu.VMEM
        DMA = pltpu.SemaphoreType.DMA
        scratch = [
            V((3, Z, 2, R, CC), BF16),
            V((X, T, DX), BF16),
            V((T, D), BF16),
            V(wqd.shape, BF16),
            V((128, D), BF16),
            V(wqn.shape, BF16), V(wqr.shape, BF16), V(wkn.shape, BF16), V(wval.shape, BF16),
            V((wval.shape[1], wval.shape[0]), BF16),
            V((woc.shape[0] + woa.shape[0], woc.shape[1]), BF16),
            V((X, nq, T), BF16),
            V((H * (NOPE + ROPE), T), BF16), V((H * (NOPE + ROPE), T), BF16),
            V((H // 2, 256, 4 * T), BF16),
            V((Z, X, nk + 2 * RX, T), BF16),
            V((ROPE, T), F32), V((2, ROPE, T), F32),
            V((nq * X, 128), F32), V((nk * X, 128), F32),
            V((T, 128), F32),
            V((H, VALUE, 2 * T), F32), V((H // 2, 1, 4 * T), F32), V((H // 2, 1, 4 * T), F32),
            V((H * VALUE + 2 * H, T), F32), V((H * VALUE + 2 * H, T), F32),
            V((T, CC), F32), V((2, 8, CC), F32), V((T, CC), F32),
            V((X, T, DX), BF16), V((X - 1, T, DX), BF16),
            DMA((13,)),
            DMA((6,)), DMA((6,)),
            DMA((3,)), DMA((3,)), DMA((1,)), DMA((1,)),
            DMA((2, K)), DMA((Z, 2)), DMA((Z,)), DMA((Z, 3)), DMA((Z, 3)),
            DMA((2, Z // 2, 2)), DMA((Z, 2)), DMA((Z,)), DMA((Z,)), DMA((1,)), DMA((1,)),
            DMA((1,)), DMA((1,)), DMA((2,)), DMA((2,)), DMA((3,)), DMA((3,)),
        ]
        return pl.pallas_call(
            functools.partial(kernel, SP, X),
            out_shape=jax.ShapeDtypeStruct((T, DX), BF16),
            in_specs=[anyspace, vmem, anyspace, anyspace, anyspace, vmem, anyspace, anyspace, anyspace,
                      vmem, vmem] + [anyspace] * 6,
            out_specs=vmem,
            scratch_shapes=scratch,
            compiler_params=pltpu.CompilerParams(
                collective_id=0, has_side_effects=True, vmem_limit_bytes=56 * 1024 * 1024
            ),
        )(
            tokens, mix_gain.reshape(1, -1), wv, wo, wi, conv_kernel, wqd, wkvd.T, wrk.T,
            q_gain.reshape(1, -1), kv_gain.reshape(1, -1), wqn, wqr, wkn, wval, woc, woa,
        )

    placed = (
        P(("grp", "sp"), "tp"),
        P(),
        P("sp", "tp"),
        P("sp", "tp"),
        P("sp", "tp"),
        P(None, "tp"),
        P(None, "tp"),
        P(None, "tp"),
        P(),
        P(),
        P(),
        P(None, "tp"),
        P(None, "tp"),
        P(None, "tp"),
        P(None, "tp"),
        P("tp", None),
        P("tp", None),
    )
    return jax.shard_map(
        per_device, mesh=mesh, in_specs=placed, out_specs=P(("grp", "sp"), "tp"), check_vma=False
    )
```

```python
import functools
import math

import jax
import jax.numpy as jnp
from jax import lax
from jax.experimental import pallas as pl
from jax.experimental.pallas import tpu as pltpu
from jax.sharding import PartitionSpec as P

NOPE = 64
ROPE = 32
VALUE = 64
EPS = 1e-06
THETA = 10000.0
LOG2E = 1.4426950408889634
MESH = pl.DeviceIdType.MESH
F32 = jnp.float32
BF16 = jnp.bfloat16
STRIDE = 3
W_FIRST = 3
W_EACH = 2


def dot_f32(a, b, contract=((1,), (0,))):
    return lax.dot_general(a, b, (contract, ((), ())), preferred_element_type=F32)


def kernel(
    SP, X,
    tokens, mix_gain, wv, wo, wi, conv_kernel, wqd, wkvd, wrk, q_gain, kv_gain,
    wqn, wqr, wkn, wval, woc, woa,
    out,
    wbuf, tok, scaled, wqd_v, wd_t, wqn_v, wqr_v, wkn_v, wval_v, wval_t, wout,
    qbuf, qmine, qpart, qz, kvbuf, kv_mine, rope_scr, cs_scr, qg_col, kvg_col, rs_scr,
    o_acc, m_acc, l_acc, o_send, o_recv, gated, halo, yconv, rs_send, rs_recv,
    loc, tk_s, tk_r, q_s, q_r, qp_s, qp_r, kf_s, kn_s, ko_s, ko_r, kh_s, kh_r, kz_r, kx_s, kx_r, wz_s, wz_r, wp_s, wp_r, wq_s, wq_r,
    o_s, o_r, h_s, h_r, r_s, r_r,
):
    Z = SP // 2
    HALF = Z // 2
    K = (HALF - 1) // STRIDE
    assert HALF == STRIDE * K + 1
    T = tokens.shape[0]
    DX = tokens.shape[1]
    D = DX * X
    H = wqn.shape[1] // NOPE
    sp = lax.axis_index("sp")
    x = lax.axis_index("tp")
    z = lax.div(sp, 2)
    c = lax.rem(sp, 2)
    def core_at(step):
        return {"sp": lax.rem(z + step + Z, Z) * 2 + c}

    xr = lax.rem(x + 1, X)
    xl = lax.rem(x + X - 1, X)
    xo = lax.rem(x + 2, X)
    to_up, to_dn = core_at(1), core_at(-1)
    far_up, far_dn = core_at(STRIDE), core_at(-STRIDE)
    partner = {"sp": z * 2 + 1 - c}
    to_xr, to_xl, to_xo = {"tp": xr}, {"tp": xl}, {"tp": xo}
    prev_sp = lax.rem(sp + SP - 1, SP)
    next_sp = lax.rem(sp + 1, SP)
    other_chip = {"sp": jnp.where(c == 0, prev_sp, next_sp)}

    def remote(src, dst, ssem, rsem, dev):
        return pltpu.make_async_remote_copy(
            src_ref=src, dst_ref=dst, send_sem=ssem, recv_sem=rsem, device_id=dev, device_id_type=MESH
        )

    local = []
    def bring(src, dst):
        cp = pltpu.make_async_copy(src, dst, loc.at[len(local)])
        local.append(cp)
        cp.start()
        return cp

    conv_cp = [bring(w, wbuf.at[i, z, c]) for i, w in enumerate((wv, wo, wi))]
    tok_cp = bring(tokens, tok.at[x])
    nk, nr = wkvd.shape[0], wrk.shape[0]
    down_cp = [bring(wqd, wqd_v), bring(wkvd, wd_t.at[pl.ds(0, nk)]), bring(wrk, wd_t.at[pl.ds(nk, nr)])]
    up_cp = [bring(wqn, wqn_v), bring(wqr, wqr_v), bring(wkn, wkn_v), bring(wval, wval_v)]
    NC = woc.shape[0]
    out_cp = [bring(woc, wout.at[pl.ds(0, NC)]), bring(woa, wout.at[pl.ds(NC, woa.shape[0])])]

    barrier = pltpu.get_barrier_semaphore()
    for dev in (to_up, to_dn, far_up, far_dn, partner, to_xr, to_xl, to_xo, other_chip):
        pl.semaphore_signal(barrier, inc=1, device_id=dev, device_id_type=MESH)
    pl.semaphore_wait(barrier, 9)

    h = T // 2
    lo, hi = pl.ds(0, h), pl.ds(h, h)

    def tok_copy(k, piece, rows, dev, first):
        src = tokens.at[rows] if first else tok.at[piece, rows]
        return remote(src, tok.at[piece, rows], tk_s.at[k], tk_r.at[k], dev)

    tok_sends = [
        tok_copy(0, x, lo, to_xr, True), tok_copy(2, x, hi, to_xl, True),
        tok_copy(1, x, hi, to_xr, True), tok_copy(3, x, lo, to_xl, True),
    ]
    for cp in tok_sends:
        cp.start()

    def w_z(slot, d, way, core, dev):
        piece = wbuf.at[:, slot, core]
        return remote(piece, piece, wz_s.at[way, d, core], wz_r.at[slot, core], dev)

    def w_p(slot):
        return remote(wbuf.at[:, slot], wbuf.at[:, slot], wp_s.at[slot], wp_r.at[slot], partner)

    def w_own(core):
        return remote(wbuf.at[:, z, core], wbuf.at[:, z, core], wq_s.at[0], wq_r.at[0], partner)

    for cp in conv_cp:
        cp.wait()
    w_own(c).start()

    def w_begin(core):
        w_z(z, 0, 0, core, to_up).start()
        w_z(z, 0, 1, core, to_dn).start()

    pl.when(c == 1)(lambda: w_begin(1))

    def w_in(k, way):
        slot = lax.rem(z - k + Z, Z) if way == 0 else lax.rem(z + k, Z)
        dev = to_up if way == 0 else to_dn
        end = HALF if way == 0 else HALF - 1
        for core in (1, 0):
            w_z(slot, k, way, core, dev).wait_recv()
            pl.when(k < end)(lambda core=core: w_z(slot, k, way, core, dev).start())
        w_p(slot).start()

    def w_step(k):
        pl.when(jnp.logical_and(c == 1, k <= HALF))(lambda: w_in(k, 0))
        pl.when(jnp.logical_and(c == 1, k <= HALF - 1))(lambda: w_in(k, 1))

    def w_steps(first, count):
        def one(i, _):
            w_step(first + i)
            return 0
        lax.fori_loop(0, count, one, 0)

    wd_t[nk + nr :, :] = jnp.zeros((wd_t.shape[0] - nk - nr, D), BF16)
    rows16 = lax.broadcasted_iota(jnp.int32, (ROPE, T), 0)
    freq = jnp.where(rows16 >= ROPE // 2, rows16 - ROPE // 2, rows16).astype(F32) * 2.0
    inverse = jnp.exp(freq * (-math.log(THETA) / ROPE))
    phase = (sp * T + lax.broadcasted_iota(jnp.int32, (ROPE, T), 1)).astype(F32) * inverse
    cs_scr[0] = jnp.cos(phase)
    cs_scr[1] = jnp.sin(phase)
    qg_col[...] = jnp.transpose(jnp.broadcast_to(q_gain[...].astype(F32), (128, q_gain.shape[1])))
    kvg_col[...] = jnp.transpose(jnp.broadcast_to(kv_gain[...].astype(F32), (128, kv_gain.shape[1])))
    qz[...] = jnp.zeros(qz.shape, BF16)
    o_acc[...] = jnp.zeros(o_acc.shape, F32)
    m_acc[...] = jnp.full(m_acc.shape, -jnp.inf, F32)
    l_acc[...] = jnp.zeros(l_acc.shape, F32)
    for cp in up_cp:
        cp.wait()
    wval_t[...] = jnp.transpose(wval_v[...].astype(F32)).astype(BF16)

    w_own(1 - c).wait_recv()
    pl.when(c == 1)(lambda: w_begin(0))
    tok_copy(0, xl, lo, to_xr, False).wait_recv()
    tok_copy(4, xl, lo, to_xr, False).start()
    tok_copy(2, xr, hi, to_xl, False).wait_recv()
    tok_copy(5, xr, hi, to_xl, False).start()
    tok_copy(1, xl, hi, to_xr, False).wait_recv()
    tok_copy(3, xr, lo, to_xl, False).wait_recv()
    w_steps(1, 1)
    tok_copy(4, xo, lo, to_xr, False).wait_recv()
    tok_copy(5, xo, hi, to_xl, False).wait_recv()
    tok_cp.wait()

    for cp in down_cp:
        cp.wait()
    down_q = jnp.zeros((T, wqd.shape[1]), F32)
    down_k = jnp.zeros((T, wd_t.shape[0]), F32)
    squares = jnp.zeros((T, 1), F32)
    for j in range(X):
        t = tok[j].astype(F32)
        s = (t * mix_gain[:, j * DX : (j + 1) * DX].astype(F32)).astype(BF16)
        scaled[:, j * DX : (j + 1) * DX] = s
        squares += jnp.sum(t * t, axis=1, keepdims=True)
        down_q += dot_f32(s, wqd_v[j * DX : (j + 1) * DX, :])
        down_k += dot_f32(s, wd_t[:, j * DX : (j + 1) * DX], ((1,), (1,)))
    row_scale = lax.rsqrt(squares / D + EPS)
    rs_scr[...] = jnp.broadcast_to(row_scale, rs_scr.shape)
    down_t = jnp.transpose(jnp.concatenate([down_q, down_k], axis=1) * row_scale)
    nq = wqd.shape[1]
    kv_mine[:nk, :] = down_t[nq : nq + nk].astype(BF16)

    def turned(v, cosine, sine):
        half = ROPE // 2
        return v * cosine + jnp.concatenate([-v[half:], v[:half]], axis=0) * sine

    raw = down_t[nq + nk : nq + nk + nr].astype(BF16).astype(F32)
    rope_scr[...] = turned(raw, cs_scr[0], cs_scr[1])
    RX = ROPE // X
    mine = rope_scr[pl.ds(pl.multiple_of(x * RX, RX), RX), :]
    kv_mine[nk:, :] = jnp.concatenate([mine, jnp.zeros((RX, T), F32)], axis=0).astype(BF16)
    k_own = remote(kv_mine, kvbuf.at[z, x, 1], ko_s.at[0], ko_r.at[0], partner)
    pl.when(c == 1)(k_own.start)

    def keep_mine():
        kvbuf[z, x, 0] = kv_mine[...]

    pl.when(c == 0)(keep_mine)

    def k_far(slot, j, way):
        piece = kvbuf.at[slot, x]
        return remote(piece, piece, kf_s.at[way, j], kz_r.at[slot], far_dn if way else far_up)

    def k_near(slot, way):
        piece = kvbuf.at[slot, x]
        return remote(piece, piece, kn_s.at[slot, way], kz_r.at[slot], to_dn if way else to_up)

    def k_x(slot, piece, kind, dev):
        return remote(kvbuf.at[slot, piece], kvbuf.at[slot, piece], kx_s.at[slot, kind], kx_r.at[slot, kind], dev)

    def k_hand(slot):
        return remote(kvbuf.at[slot, :, 1], kvbuf.at[slot, :, 1], kh_s.at[slot], kh_r.at[slot], partner)

    def k_begin():
        k_own.wait_recv()
        k_far(z, 0, 0).start()
        k_far(z, 0, 1).start()
        k_near(z, 0).start()
        k_near(z, 1).start()
        k_x(z, x, 0, to_xr).start()
        k_x(z, x, 1, to_xl).start()


    qbuf[x] = down_t[:nq].astype(BF16)

    def q_copy(kind, piece, dev):
        return remote(qbuf.at[piece], qbuf.at[piece], q_s.at[kind], q_r.at[kind], dev)

    q_sends = [q_copy(2, x, to_xo), q_copy(0, x, to_xr), q_copy(1, x, to_xl)]
    for cp in q_sends:
        cp.start()
    pl.when(c == 0)(k_begin)
    w_steps(2, W_FIRST - 1)

    factor = (NOPE + ROPE) ** (-0.5) * LOG2E
    q_exchange = remote(qmine, qpart, qp_s.at[0], qp_r.at[0], partner)

    def make_q():
        q_copy(0, xl, to_xr).wait_recv()
        q_copy(1, xr, to_xl).wait_recv()
        q_copy(2, xo, to_xo).wait_recv()
        qf = qbuf[...].reshape(X * nq, T).astype(F32)
        scale = lax.rsqrt(jnp.mean(qf * qf, axis=0, keepdims=True) + EPS)
        qn = (qf * scale * qg_col[...]).astype(BF16)
        nope = dot_f32(wqn_v[...], qn, ((0,), (0,))) * factor
        qmine[: H * NOPE, :] = nope.astype(BF16)
        rope = dot_f32(wqr_v[...], qn, ((0,), (0,)))
        for i in range(H):
            r = turned(rope[i * ROPE : (i + 1) * ROPE], cs_scr[0], cs_scr[1]) * factor
            qmine[H * NOPE + i * ROPE : H * NOPE + (i + 1) * ROPE, :] = r.astype(BF16)
        q_exchange.start()

    def place_q():
        q_exchange.wait_recv()
        for i in range(H):
            p, e = divmod(i, 2)
            for src, at in ((qmine, 0), (qpart, T)):
                cols = slice(e * 2 * T + at, e * 2 * T + at + T)
                qz[p, e * NOPE : (e + 1) * NOPE, cols] = src[i * NOPE : (i + 1) * NOPE, :]
                qz[p, 2 * NOPE : 2 * NOPE + ROPE, cols] = src[H * NOPE + i * ROPE : H * NOPE + (i + 1) * ROPE, :]

    def keys(slot):
        lat = kvbuf[slot, :, c, :nk, :].reshape(X * nk, T).astype(F32)
        rope = kvbuf[slot, :, c, nk : nk + 2 * RX, :].astype(F32)[:, :RX].reshape(ROPE, T)
        return lat, rope

    def chunk(slot_a, slot_b):
        la, ra = keys(slot_a)
        lb, rb = keys(slot_b)
        lat = jnp.concatenate([la, lb], axis=1)
        scale = lax.rsqrt(jnp.mean(lat * lat, axis=0, keepdims=True) + EPS)
        gain = kvg_col[...]
        n = (lat * scale * jnp.concatenate([gain, gain], axis=1)).astype(BF16)
        kn = dot_f32(n, wkn_v[...], ((0,), (0,))).astype(BF16)
        rope = jnp.concatenate([ra, rb], axis=1)
        kr = jnp.transpose(jnp.concatenate([rope, jnp.zeros((128 - ROPE, 2 * T), F32)], axis=0)).astype(BF16)
        vt = dot_f32(wval_t[...], n).astype(BF16)
        for p in range(H // 2):
            kp = jnp.concatenate([kn[:, p * 128 : (p + 1) * 128], kr], axis=1)
            s = dot_f32(kp, qz[p])
            old = m_acc[p]
            new = jnp.maximum(old, jnp.max(s, axis=0, keepdims=True))
            m_acc[p] = new
            fade = jnp.exp2(old - new)
            w = jnp.exp2(s - new)
            l_acc[p] = l_acc[p] * fade + jnp.sum(w, axis=0, keepdims=True)
            wb = w.astype(BF16)
            for e in range(2):
                i = 2 * p + e
                cols = slice(e * 2 * T, (e + 1) * 2 * T)
                o_acc[i] = o_acc[i] * fade[:, cols] + dot_f32(vt[i * VALUE : (i + 1) * VALUE], wb[:, cols])

    def halo_copy(k, dev):
        rows = pl.ds(0, 8) if k == 1 else pl.ds(T - 8, 8)
        return remote(gated.at[rows], halo.at[k], h_s.at[k], h_r.at[k], dev)

    to_next, to_prev = {"sp": next_sp}, {"sp": prev_sp}

    def conv_gates():
        def got(i, _):
            w_p(lax.rem(z + i, Z)).wait_recv()
            return 0

        def all_in():
            lax.fori_loop(1, Z, got, 0)

        pl.when(c == 0)(all_in)

        def project(i):
            w = wbuf[i].reshape(D, wbuf.shape[-1])
            return (dot_f32(scaled[...], w) * rs_scr[:, 0:1]).astype(BF16).astype(F32)
        inner = project(2)
        value = project(0)
        gated[...] = (inner * value).astype(BF16).astype(F32)
        halo_copy(0, to_next).start()
        halo_copy(1, to_prev).start()
        yconv[...] = project(1)

    def at(offset):
        return lax.rem(z + offset + 2 * Z, Z)

    def spread(slot):
        k_x(slot, x, 0, to_xr).start()
        k_x(slot, x, 1, to_xl).start()

    def stop(j, way):
        slot = at(STRIDE * j if way else -STRIDE * j)
        k_near(slot, 0).wait_recv()
        pl.when(j < K)(lambda: k_far(slot, j, way).start())
        if way == 0:
            k_near(slot, 0).start()
            k_near(slot, 1).start()
        else:
            k_near(slot, 0).start()
            pl.when(j < K)(lambda: k_near(slot, 1).start())
        spread(slot)

    def leaf(slot):
        k_near(slot, 0).wait_recv()
        spread(slot)

    def relay_up(slot):
        k_x(slot, xl, 0, to_xr).wait_recv()
        k_x(slot, xl, 2, to_xr).start()

    def relay_dn(slot):
        k_x(slot, xr, 1, to_xl).wait_recv()
        k_x(slot, xr, 2, to_xl).start()

    def leaves(j, fn_up, fn_dn):
        def inner():
            fn_up(at(-STRIDE * j + 1))
            fn_dn(at(STRIDE * j - 1))

        fn_up(at(-STRIDE * j - 1))
        pl.when(j < K)(lambda: fn_dn(at(STRIDE * j + 1)))
        pl.when(j >= 1)(inner)

    def got_up(slot):
        k_x(slot, xr, 1, to_xl).wait_recv()
        k_x(slot, xo, 2, to_xr).wait_recv()

    def got_dn(slot):
        k_x(slot, xl, 0, to_xr).wait_recv()
        k_x(slot, xo, 2, to_xl).wait_recv()

    def pair(j, r):
        off = STRIDE * j + jnp.where(r == 0, 0, jnp.where(r == 1, -1, 1))
        own = off == HALF
        slot_a = at(-off)
        slot_b = jnp.where(own, z, at(off))

        def take():
            got_up(slot_a)
            pl.when(own)(lambda: got_up(slot_b))
            pl.when(jnp.logical_not(own))(lambda: got_dn(slot_b))
            k_hand(slot_a).start()
            k_hand(slot_b).start()

        def handed():
            k_hand(slot_a).wait_recv()
            k_hand(slot_b).wait_recv()

        pl.when(c == 0)(take)
        pl.when(c == 1)(handed)
        chunk(slot_a, slot_b)

    def transport(i):
        def stops_in():
            stop(i, 0)
            stop(i, 1)

        pl.when(i <= K)(stops_in)
        pl.when(i - 1 <= K)(lambda: leaves(i - 1, leaf, leaf))

        def relay_stops():
            relay_up(at(-STRIDE * (i - 1)))
            pl.when(i - 1 >= 1)(lambda: relay_dn(at(STRIDE * (i - 1))))

        pl.when(i - 1 <= K)(relay_stops)
        pl.when(jnp.logical_and(i - 2 >= 0, i - 2 <= K))(lambda: leaves(i - 2, relay_up, relay_dn))

    def step(i, _):
        pl.when(c == 0)(lambda: transport(i))
        pl.when(i <= K + 1)(lambda: w_steps(W_FIRST + 1 + W_EACH * (i - 1), W_EACH))
        pl.when(i == 1)(make_q)
        pl.when(i == 2)(place_q)
        pl.when(i == K + 2)(w_rest)

        def one(r, _):
            j = jnp.where(r == 0, i - 2, i - 3)
            here = jnp.logical_and(j >= jnp.where(r == 2, 0, 1), j <= K)
            pl.when(here)(lambda: pair(j, r))
            return 0

        lax.fori_loop(0, 3, one, 0)
        return 0

    def w_rest():
        w_steps(W_FIRST + 1 + W_EACH * (K + 1), HALF - W_FIRST - W_EACH * (K + 1))
        conv_gates()

    lax.fori_loop(1, K + 4, step, 0)

    for i in range(H):
        p, e = divmod(i, 2)
        theirs = slice(e * 2 * T + T, (e + 1) * 2 * T)
        o_send[i * VALUE : (i + 1) * VALUE, :] = o_acc[i][:, T:]
        o_send[H * VALUE + i : H * VALUE + i + 1, :] = m_acc[p][:, theirs]
        o_send[H * VALUE + H + i : H * VALUE + H + i + 1, :] = l_acc[p][:, theirs]
    o_exchange = remote(o_send, o_recv, o_s.at[0], o_r.at[0], partner)
    o_exchange.start()

    halo_copy(0, to_next).wait_recv()
    halo_copy(1, to_prev).wait_recv()
    g = gated[...]
    row = lax.broadcasted_iota(jnp.int32, g.shape, 0)
    before = jnp.where(sp == 0, 0.0, halo[0, 7:8, :])
    after = jnp.where(sp == SP - 1, 0.0, halo[1, 0:1, :])
    g_before = jnp.where(row == 0, before, pltpu.roll(g, 1, 0))
    g_after = jnp.where(row == T - 1, after, pltpu.roll(g, T - 1, 0))
    taps = conv_kernel[...].astype(F32)
    conv = g_before * taps[0:1] + g * taps[1:2] + g_after * taps[2:3]
    y_conv = (yconv[...] * conv).astype(BF16)

    o_exchange.wait_recv()
    parts = []
    for i in range(H):
        p, e = divmod(i, 2)
        ours = slice(e * 2 * T, e * 2 * T + T)
        m1 = m_acc[p][:, ours]
        m2 = o_recv[H * VALUE + i : H * VALUE + i + 1, :]
        top = jnp.maximum(m1, m2)
        a1, a2 = jnp.exp2(m1 - top), jnp.exp2(m2 - top)
        total = a1 * l_acc[p][:, ours] + a2 * o_recv[H * VALUE + H + i : H * VALUE + H + i + 1, :]
        summed = a1 * o_acc[i][:, :T] + a2 * o_recv[i * VALUE : (i + 1) * VALUE, :]
        parts.append(summed / total)
    y_attn = jnp.transpose(jnp.concatenate(parts, axis=0)).astype(BF16)
    y = jnp.concatenate([y_conv, y_attn], axis=1)
    for cp in out_cp:
        cp.wait()
    for rel, dev in ((2, to_xo), (1, to_xr), (3, to_xl), (0, None)):
        dest = lax.rem(x + rel, X)
        cols = pl.ds(pl.multiple_of(dest * DX, DX), DX)
        rs_send[rel] = dot_f32(y, wout[:, cols]).astype(BF16)
        if dev is not None:
            remote(rs_send.at[rel], rs_recv.at[rel - 1], r_s.at[rel - 1], r_r.at[rel - 1], dev).start()
    total = rs_send[0].astype(F32)
    r_copies = [
        remote(rs_send.at[rel], rs_recv.at[rel - 1], r_s.at[rel - 1], r_r.at[rel - 1], dev)
        for rel, dev in ((1, to_xr), (3, to_xl), (2, to_xo))
    ]
    for rel, cp in zip((1, 3, 2), r_copies):
        cp.wait_recv()
        total += rs_recv[rel - 1].astype(F32)
    out[...] = total.astype(BF16)

    for cp in tok_sends + [tok_copy(4, xl, lo, to_xr, False), tok_copy(5, xr, hi, to_xl, False)]:
        cp.wait_send()
    for cp in q_sends + [q_exchange, halo_copy(0, to_next), halo_copy(1, to_prev), o_exchange] + r_copies:
        cp.wait_send()

    w_own(c).wait_send()

    def w_sent(d, _):
        for core in (0, 1):
            w_z(z, d, 0, core, to_up).wait_send()

        def back():
            for core in (0, 1):
                w_z(z, d, 1, core, to_dn).wait_send()

        pl.when(d < HALF - 1)(back)
        return 0

    def w_handed(i, _):
        w_p(lax.rem(z + i, Z)).wait_send()
        return 0

    def w_all():
        lax.fori_loop(0, HALF, w_sent, 0)
        lax.fori_loop(1, Z, w_handed, 0)

    pl.when(c == 1)(w_all)

    def k_sent(j, _):
        for way in (0, 1):
            pl.when(j < K)(lambda way=way: k_far(z, j, way).wait_send())
        k_near(at(-STRIDE * j), 0).wait_send()
        k_near(at(-STRIDE * j), 1).wait_send()

        def back():
            k_near(at(STRIDE * j), 0).wait_send()
            pl.when(j < K)(lambda: k_near(at(STRIDE * j), 1).wait_send())

        pl.when(j >= 1)(back)
        return 0

    def sent_slots(s, _):
        for kind, dev in ((0, to_xr), (1, to_xl), (2, to_xr)):
            k_x(s, x, kind, dev).wait_send()
        k_hand(s).wait_send()
        return 0

    def k_all():
        lax.fori_loop(0, K + 1, k_sent, 0)
        lax.fori_loop(0, Z, sent_slots, 0)

    pl.when(c == 0)(k_all)
    pl.when(c == 1)(k_own.wait_send)


def solution(mesh):
    SP, X = mesh.shape["sp"], mesh.shape["tp"]

    def per_device(
        tokens, mix_gain, wv, wo, wi, conv_kernel, wqd, wkvd, wrk, q_gain, kv_gain,
        wqn, wqr, wkn, wval, woc, woa,
    ):
        T, DX = tokens.shape
        D = DX * X
        Z = SP // 2
        R, CC = wv.shape
        H = wqn.shape[1] // NOPE
        nk, nq = wkvd.shape[1], wqd.shape[1]
        K = (Z // 2 - 1) // STRIDE
        RX = ROPE // X
        anyspace = pl.BlockSpec(memory_space=pl.ANY)
        vmem = pl.BlockSpec(memory_space=pltpu.VMEM)
        V = pltpu.VMEM
        DMA = pltpu.SemaphoreType.DMA
        scratch = [
            V((3, Z, 2, R, CC), BF16),
            V((X, T, DX), BF16),
            V((T, D), BF16),
            V(wqd.shape, BF16),
            V((128, D), BF16),
            V(wqn.shape, BF16), V(wqr.shape, BF16), V(wkn.shape, BF16), V(wval.shape, BF16),
            V((wval.shape[1], wval.shape[0]), BF16),
            V((woc.shape[0] + woa.shape[0], woc.shape[1]), BF16),
            V((X, nq, T), BF16),
            V((H * (NOPE + ROPE), T), BF16), V((H * (NOPE + ROPE), T), BF16),
            V((H // 2, 256, 4 * T), BF16),
            V((Z, X, 2, nk + 2 * RX, T), BF16), V((nk + 2 * RX, T), BF16),
            V((ROPE, T), F32), V((2, ROPE, T), F32),
            V((nq * X, 128), F32), V((nk * X, 128), F32),
            V((T, 128), F32),
            V((H, VALUE, 2 * T), F32), V((H // 2, 1, 4 * T), F32), V((H // 2, 1, 4 * T), F32),
            V((H * VALUE + 2 * H, T), F32), V((H * VALUE + 2 * H, T), F32),
            V((T, CC), F32), V((2, 8, CC), F32), V((T, CC), F32),
            V((X, T, DX), BF16), V((X - 1, T, DX), BF16),
            DMA((13,)),
            DMA((6,)), DMA((6,)),
            DMA((3,)), DMA((3,)), DMA((1,)), DMA((1,)),
            DMA((2, K)), DMA((Z, 2)), DMA((1,)), DMA((1,)), DMA((Z,)), DMA((Z,)), DMA((Z,)), DMA((Z, 3)), DMA((Z, 3)),
            DMA((2, Z // 2, 2)), DMA((Z, 2)), DMA((Z,)), DMA((Z,)), DMA((1,)), DMA((1,)),
            DMA((1,)), DMA((1,)), DMA((2,)), DMA((2,)), DMA((3,)), DMA((3,)),
        ]
        return pl.pallas_call(
            functools.partial(kernel, SP, X),
            out_shape=jax.ShapeDtypeStruct((T, DX), BF16),
            in_specs=[anyspace, vmem, anyspace, anyspace, anyspace, vmem, anyspace, anyspace, anyspace,
                      vmem, vmem] + [anyspace] * 6,
            out_specs=vmem,
            scratch_shapes=scratch,
            compiler_params=pltpu.CompilerParams(
                collective_id=0, has_side_effects=True, vmem_limit_bytes=56 * 1024 * 1024
            ),
        )(
            tokens, mix_gain.reshape(1, -1), wv, wo, wi, conv_kernel, wqd, wkvd.T, wrk.T,
            q_gain.reshape(1, -1), kv_gain.reshape(1, -1), wqn, wqr, wkn, wval, woc, woa,
        )

    placed = (
        P(("grp", "sp"), "tp"),
        P(),
        P("sp", "tp"),
        P("sp", "tp"),
        P("sp", "tp"),
        P(None, "tp"),
        P(None, "tp"),
        P(None, "tp"),
        P(),
        P(),
        P(),
        P(None, "tp"),
        P(None, "tp"),
        P(None, "tp"),
        P(None, "tp"),
        P("tp", None),
        P("tp", None),
    )
    return jax.shard_map(
        per_device, mesh=mesh, in_specs=placed, out_specs=P(("grp", "sp"), "tp"), check_vma=False
    )
```

```python
import functools
import math

import jax
import jax.numpy as jnp
from jax import lax
from jax.experimental import pallas as pl
from jax.experimental.pallas import tpu as pltpu
from jax.sharding import PartitionSpec as P

NOPE = 64
ROPE = 32
VALUE = 64
EPS = 1e-06
THETA = 10000.0
LOG2E = 1.4426950408889634
MESH = pl.DeviceIdType.MESH
F32 = jnp.float32
BF16 = jnp.bfloat16
STRIDE = 3


def dot_f32(a, b, contract=((1,), (0,))):
    return lax.dot_general(a, b, (contract, ((), ())), preferred_element_type=F32)


def kernel(
    SP, X,
    tokens, mix_gain, wv, wo, wi, conv_kernel, wqd, wkvd, wrk, q_gain, kv_gain,
    wqn, wqr, wkn, wval, woc, woa,
    out,
    wbuf, tok, scaled, wqd_v, wd_t, wqn_v, wqr_v, wkn_v, wval_v, wval_t, wout,
    qbuf, qmine, qpart, qz, kvbuf, kv_mine, rope_scr, cs_scr, qg_col, kvg_col, rs_scr,
    o_acc, m_acc, l_acc, o_send, o_recv, gated, halo, yconv, rs_send, rs_recv,
    loc, tk_s, tk_r, q_s, q_r, qp_s, qp_r, kf_s, kn_s, ko_s, ko_r, kh_s, kh_r, kz_r, kx_s, kx_r, wf_s, wn_s, wz_r, wp_s, wp_r, wq_s, wq_r,
    o_s, o_r, h_s, h_r, r_s, r_r,
):
    Z = SP // 2
    HALF = Z // 2
    K = (HALF - 1) // STRIDE
    assert HALF == STRIDE * K + 1
    T = tokens.shape[0]
    DX = tokens.shape[1]
    D = DX * X
    H = wqn.shape[1] // NOPE
    sp = lax.axis_index("sp")
    x = lax.axis_index("tp")
    z = lax.div(sp, 2)
    c = lax.rem(sp, 2)
    def core_at(step):
        return {"sp": lax.rem(z + step + Z, Z) * 2 + c}

    xr = lax.rem(x + 1, X)
    xl = lax.rem(x + X - 1, X)
    xo = lax.rem(x + 2, X)
    to_up, to_dn = core_at(1), core_at(-1)
    far_up, far_dn = core_at(STRIDE), core_at(-STRIDE)
    partner = {"sp": z * 2 + 1 - c}
    to_xr, to_xl, to_xo = {"tp": xr}, {"tp": xl}, {"tp": xo}
    prev_sp = lax.rem(sp + SP - 1, SP)
    next_sp = lax.rem(sp + 1, SP)
    other_chip = {"sp": jnp.where(c == 0, prev_sp, next_sp)}

    def remote(src, dst, ssem, rsem, dev):
        return pltpu.make_async_remote_copy(
            src_ref=src, dst_ref=dst, send_sem=ssem, recv_sem=rsem, device_id=dev, device_id_type=MESH
        )

    local = []
    def bring(src, dst):
        cp = pltpu.make_async_copy(src, dst, loc.at[len(local)])
        local.append(cp)
        cp.start()
        return cp

    conv_cp = [bring(w, wbuf.at[i, z, c]) for i, w in enumerate((wv, wo, wi))]
    tok_cp = bring(tokens, tok.at[x])
    nk, nr = wkvd.shape[0], wrk.shape[0]
    down_cp = [bring(wqd, wqd_v), bring(wkvd, wd_t.at[pl.ds(0, nk)]), bring(wrk, wd_t.at[pl.ds(nk, nr)])]
    up_cp = [bring(wqn, wqn_v), bring(wqr, wqr_v), bring(wkn, wkn_v), bring(wval, wval_v)]
    NC = woc.shape[0]
    out_cp = [bring(woc, wout.at[pl.ds(0, NC)]), bring(woa, wout.at[pl.ds(NC, woa.shape[0])])]

    barrier = pltpu.get_barrier_semaphore()
    for dev in (to_up, to_dn, far_up, far_dn, partner, to_xr, to_xl, to_xo, other_chip):
        pl.semaphore_signal(barrier, inc=1, device_id=dev, device_id_type=MESH)
    pl.semaphore_wait(barrier, 9)

    h = T // 2
    lo, hi = pl.ds(0, h), pl.ds(h, h)

    def tok_copy(k, piece, rows, dev, first):
        src = tokens.at[rows] if first else tok.at[piece, rows]
        return remote(src, tok.at[piece, rows], tk_s.at[k], tk_r.at[k], dev)

    tok_sends = [
        tok_copy(0, x, lo, to_xr, True), tok_copy(2, x, hi, to_xl, True),
        tok_copy(1, x, hi, to_xr, True), tok_copy(3, x, lo, to_xl, True),
    ]
    for cp in tok_sends:
        cp.start()

    def at(offset):
        return lax.rem(z + offset + 2 * Z, Z)

    def leaves(j, fn_up, fn_dn):
        def inner():
            fn_up(at(-STRIDE * j + 1))
            fn_dn(at(STRIDE * j - 1))

        fn_up(at(-STRIDE * j - 1))
        pl.when(j < K)(lambda: fn_dn(at(STRIDE * j + 1)))
        pl.when(j >= 1)(inner)

    def w_far(slot, j, way, core):
        piece = wbuf.at[:, slot, core]
        return remote(piece, piece, wf_s.at[way, j, core], wz_r.at[slot, core], far_dn if way else far_up)

    def w_near(slot, way, core):
        piece = wbuf.at[:, slot, core]
        return remote(piece, piece, wn_s.at[slot, way, core], wz_r.at[slot, core], to_dn if way else to_up)

    def w_p(slot):
        return remote(wbuf.at[:, slot], wbuf.at[:, slot], wp_s.at[slot], wp_r.at[slot], partner)

    def w_own(core):
        return remote(wbuf.at[:, z, core], wbuf.at[:, z, core], wq_s.at[0], wq_r.at[0], partner)

    for cp in conv_cp:
        cp.wait()
    w_own(c).start()

    def w_begin(core):
        for way in (0, 1):
            w_far(z, 0, way, core).start()
        for way in (0, 1):
            w_near(z, way, core).start()

    pl.when(c == 1)(lambda: w_begin(1))

    def w_stop(j, way):
        slot = at(STRIDE * j if way else -STRIDE * j)
        for core in (1, 0):
            w_near(slot, 0, core).wait_recv()
            pl.when(j < K)(lambda core=core: w_far(slot, j, way, core).start())

        def nears(to):
            for core in (1, 0):
                w_near(slot, to, core).start()

        nears(0)
        if way == 0:
            nears(1)
        else:
            pl.when(j < K)(lambda: nears(1))
        w_p(slot).start()

    def w_leaf(slot):
        for core in (1, 0):
            w_near(slot, 0, core).wait_recv()
        w_p(slot).start()

    def w_step(j):
        def stops_in():
            w_stop(j, 0)
            w_stop(j, 1)

        pl.when(jnp.logical_and(c == 1, j <= K))(stops_in)
        pl.when(jnp.logical_and(c == 1, j <= K + 1))(lambda: leaves(j - 1, w_leaf, w_leaf))

    wd_t[nk + nr :, :] = jnp.zeros((wd_t.shape[0] - nk - nr, D), BF16)
    rows16 = lax.broadcasted_iota(jnp.int32, (ROPE, T), 0)
    freq = jnp.where(rows16 >= ROPE // 2, rows16 - ROPE // 2, rows16).astype(F32) * 2.0
    inverse = jnp.exp(freq * (-math.log(THETA) / ROPE))
    phase = (sp * T + lax.broadcasted_iota(jnp.int32, (ROPE, T), 1)).astype(F32) * inverse
    cs_scr[0] = jnp.cos(phase)
    cs_scr[1] = jnp.sin(phase)
    qg_col[...] = jnp.transpose(jnp.broadcast_to(q_gain[...].astype(F32), (128, q_gain.shape[1])))
    kvg_col[...] = jnp.transpose(jnp.broadcast_to(kv_gain[...].astype(F32), (128, kv_gain.shape[1])))
    qz[...] = jnp.zeros(qz.shape, BF16)
    o_acc[...] = jnp.zeros(o_acc.shape, F32)
    m_acc[...] = jnp.full(m_acc.shape, -jnp.inf, F32)
    l_acc[...] = jnp.zeros(l_acc.shape, F32)
    for cp in up_cp:
        cp.wait()
    wval_t[...] = jnp.transpose(wval_v[...].astype(F32)).astype(BF16)

    w_own(1 - c).wait_recv()
    pl.when(c == 1)(lambda: w_begin(0))
    tok_copy(0, xl, lo, to_xr, False).wait_recv()
    tok_copy(4, xl, lo, to_xr, False).start()
    tok_copy(2, xr, hi, to_xl, False).wait_recv()
    tok_copy(5, xr, hi, to_xl, False).start()
    tok_copy(1, xl, hi, to_xr, False).wait_recv()
    tok_copy(3, xr, lo, to_xl, False).wait_recv()
    w_step(1)
    tok_copy(4, xo, lo, to_xr, False).wait_recv()
    tok_copy(5, xo, hi, to_xl, False).wait_recv()
    tok_cp.wait()

    for cp in down_cp:
        cp.wait()
    down_q = jnp.zeros((T, wqd.shape[1]), F32)
    down_k = jnp.zeros((T, wd_t.shape[0]), F32)
    squares = jnp.zeros((T, 1), F32)
    for j in range(X):
        t = tok[j].astype(F32)
        s = (t * mix_gain[:, j * DX : (j + 1) * DX].astype(F32)).astype(BF16)
        scaled[:, j * DX : (j + 1) * DX] = s
        squares += jnp.sum(t * t, axis=1, keepdims=True)
        down_q += dot_f32(s, wqd_v[j * DX : (j + 1) * DX, :])
        down_k += dot_f32(s, wd_t[:, j * DX : (j + 1) * DX], ((1,), (1,)))
    row_scale = lax.rsqrt(squares / D + EPS)
    rs_scr[...] = jnp.broadcast_to(row_scale, rs_scr.shape)
    down_t = jnp.transpose(jnp.concatenate([down_q, down_k], axis=1) * row_scale)
    nq = wqd.shape[1]
    kv_mine[:nk, :] = down_t[nq : nq + nk].astype(BF16)

    def turned(v, cosine, sine):
        half = ROPE // 2
        return v * cosine + jnp.concatenate([-v[half:], v[:half]], axis=0) * sine

    raw = down_t[nq + nk : nq + nk + nr].astype(BF16).astype(F32)
    rope_scr[...] = turned(raw, cs_scr[0], cs_scr[1])
    RX = ROPE // X
    mine = rope_scr[pl.ds(pl.multiple_of(x * RX, RX), RX), :]
    kv_mine[nk:, :] = jnp.concatenate([mine, jnp.zeros((RX, T), F32)], axis=0).astype(BF16)
    k_own = remote(kv_mine, kvbuf.at[z, x, 1], ko_s.at[0], ko_r.at[0], partner)
    pl.when(c == 1)(k_own.start)

    def keep_mine():
        kvbuf[z, x, 0] = kv_mine[...]

    pl.when(c == 0)(keep_mine)

    def k_far(slot, j, way):
        piece = kvbuf.at[slot, x]
        return remote(piece, piece, kf_s.at[way, j], kz_r.at[slot], far_dn if way else far_up)

    def k_near(slot, way):
        piece = kvbuf.at[slot, x]
        return remote(piece, piece, kn_s.at[slot, way], kz_r.at[slot], to_dn if way else to_up)

    def k_x(slot, piece, kind, dev):
        return remote(kvbuf.at[slot, piece], kvbuf.at[slot, piece], kx_s.at[slot, kind], kx_r.at[slot, kind], dev)

    def k_hand(slot):
        return remote(kvbuf.at[slot, :, 1], kvbuf.at[slot, :, 1], kh_s.at[slot], kh_r.at[slot], partner)

    def k_begin():
        k_own.wait_recv()
        k_far(z, 0, 0).start()
        k_far(z, 0, 1).start()
        k_near(z, 0).start()
        k_near(z, 1).start()
        k_x(z, x, 0, to_xr).start()
        k_x(z, x, 1, to_xl).start()


    qbuf[x] = down_t[:nq].astype(BF16)

    def q_copy(kind, piece, dev):
        return remote(qbuf.at[piece], qbuf.at[piece], q_s.at[kind], q_r.at[kind], dev)

    q_sends = [q_copy(2, x, to_xo), q_copy(0, x, to_xr), q_copy(1, x, to_xl)]
    for cp in q_sends:
        cp.start()
    pl.when(c == 0)(k_begin)
    w_step(2)

    factor = (NOPE + ROPE) ** (-0.5) * LOG2E
    q_exchange = remote(qmine, qpart, qp_s.at[0], qp_r.at[0], partner)

    def make_q():
        q_copy(0, xl, to_xr).wait_recv()
        q_copy(1, xr, to_xl).wait_recv()
        q_copy(2, xo, to_xo).wait_recv()
        qf = qbuf[...].reshape(X * nq, T).astype(F32)
        scale = lax.rsqrt(jnp.mean(qf * qf, axis=0, keepdims=True) + EPS)
        qn = (qf * scale * qg_col[...]).astype(BF16)
        nope = dot_f32(wqn_v[...], qn, ((0,), (0,))) * factor
        qmine[: H * NOPE, :] = nope.astype(BF16)
        rope = dot_f32(wqr_v[...], qn, ((0,), (0,)))
        for i in range(H):
            r = turned(rope[i * ROPE : (i + 1) * ROPE], cs_scr[0], cs_scr[1]) * factor
            qmine[H * NOPE + i * ROPE : H * NOPE + (i + 1) * ROPE, :] = r.astype(BF16)
        q_exchange.start()

    def place_q():
        q_exchange.wait_recv()
        for i in range(H):
            p, e = divmod(i, 2)
            for src, at in ((qmine, 0), (qpart, T)):
                cols = slice(e * 2 * T + at, e * 2 * T + at + T)
                qz[p, e * NOPE : (e + 1) * NOPE, cols] = src[i * NOPE : (i + 1) * NOPE, :]
                qz[p, 2 * NOPE : 2 * NOPE + ROPE, cols] = src[H * NOPE + i * ROPE : H * NOPE + (i + 1) * ROPE, :]

    def keys(slot):
        lat = kvbuf[slot, :, c, :nk, :].reshape(X * nk, T).astype(F32)
        rope = kvbuf[slot, :, c, nk : nk + 2 * RX, :].astype(F32)[:, :RX].reshape(ROPE, T)
        return lat, rope

    def chunk(slot_a, slot_b):
        la, ra = keys(slot_a)
        lb, rb = keys(slot_b)
        lat = jnp.concatenate([la, lb], axis=1)
        scale = lax.rsqrt(jnp.mean(lat * lat, axis=0, keepdims=True) + EPS)
        gain = kvg_col[...]
        n = (lat * scale * jnp.concatenate([gain, gain], axis=1)).astype(BF16)
        kn = dot_f32(n, wkn_v[...], ((0,), (0,))).astype(BF16)
        rope = jnp.concatenate([ra, rb], axis=1)
        kr = jnp.transpose(jnp.concatenate([rope, jnp.zeros((128 - ROPE, 2 * T), F32)], axis=0)).astype(BF16)
        vt = dot_f32(wval_t[...], n).astype(BF16)
        for p in range(H // 2):
            kp = jnp.concatenate([kn[:, p * 128 : (p + 1) * 128], kr], axis=1)
            s = dot_f32(kp, qz[p])
            old = m_acc[p]
            new = jnp.maximum(old, jnp.max(s, axis=0, keepdims=True))
            m_acc[p] = new
            fade = jnp.exp2(old - new)
            w = jnp.exp2(s - new)
            l_acc[p] = l_acc[p] * fade + jnp.sum(w, axis=0, keepdims=True)
            wb = w.astype(BF16)
            for e in range(2):
                i = 2 * p + e
                cols = slice(e * 2 * T, (e + 1) * 2 * T)
                o_acc[i] = o_acc[i] * fade[:, cols] + dot_f32(vt[i * VALUE : (i + 1) * VALUE], wb[:, cols])

    def halo_copy(k, dev):
        rows = pl.ds(0, 8) if k == 1 else pl.ds(T - 8, 8)
        return remote(gated.at[rows], halo.at[k], h_s.at[k], h_r.at[k], dev)

    to_next, to_prev = {"sp": next_sp}, {"sp": prev_sp}

    def conv_gates():
        def got(i, _):
            w_p(lax.rem(z + i, Z)).wait_recv()
            return 0

        def all_in():
            lax.fori_loop(1, Z, got, 0)

        pl.when(c == 0)(all_in)

        def project(i):
            w = wbuf[i].reshape(D, wbuf.shape[-1])
            return (dot_f32(scaled[...], w) * rs_scr[:, 0:1]).astype(BF16).astype(F32)
        inner = project(2)
        value = project(0)
        gated[...] = (inner * value).astype(BF16).astype(F32)
        halo_copy(0, to_next).start()
        halo_copy(1, to_prev).start()
        yconv[...] = project(1)

    def spread(slot):
        k_x(slot, x, 0, to_xr).start()
        k_x(slot, x, 1, to_xl).start()

    def stop(j, way):
        slot = at(STRIDE * j if way else -STRIDE * j)
        k_near(slot, 0).wait_recv()
        pl.when(j < K)(lambda: k_far(slot, j, way).start())
        if way == 0:
            k_near(slot, 0).start()
            k_near(slot, 1).start()
        else:
            k_near(slot, 0).start()
            pl.when(j < K)(lambda: k_near(slot, 1).start())
        spread(slot)

    def leaf(slot):
        k_near(slot, 0).wait_recv()
        spread(slot)

    def relay_up(slot):
        k_x(slot, xl, 0, to_xr).wait_recv()
        k_x(slot, xl, 2, to_xr).start()

    def relay_dn(slot):
        k_x(slot, xr, 1, to_xl).wait_recv()
        k_x(slot, xr, 2, to_xl).start()

    def got_up(slot):
        k_x(slot, xr, 1, to_xl).wait_recv()
        k_x(slot, xo, 2, to_xr).wait_recv()

    def got_dn(slot):
        k_x(slot, xl, 0, to_xr).wait_recv()
        k_x(slot, xo, 2, to_xl).wait_recv()

    def pair(j, r):
        off = STRIDE * j + jnp.where(r == 0, 0, jnp.where(r == 1, -1, 1))
        own = off == HALF
        slot_a = at(-off)
        slot_b = jnp.where(own, z, at(off))

        def take():
            got_up(slot_a)
            pl.when(own)(lambda: got_up(slot_b))
            pl.when(jnp.logical_not(own))(lambda: got_dn(slot_b))
            k_hand(slot_a).start()
            k_hand(slot_b).start()

        def handed():
            k_hand(slot_a).wait_recv()
            k_hand(slot_b).wait_recv()

        pl.when(c == 0)(take)
        pl.when(c == 1)(handed)
        chunk(slot_a, slot_b)

    def transport(i):
        def stops_in():
            stop(i, 0)
            stop(i, 1)

        pl.when(i <= K)(stops_in)
        pl.when(i - 1 <= K)(lambda: leaves(i - 1, leaf, leaf))

        def relay_stops():
            relay_up(at(-STRIDE * (i - 1)))
            pl.when(i - 1 >= 1)(lambda: relay_dn(at(STRIDE * (i - 1))))

        pl.when(i - 1 <= K)(relay_stops)
        pl.when(jnp.logical_and(i - 2 >= 0, i - 2 <= K))(lambda: leaves(i - 2, relay_up, relay_dn))

    def step(i, _):
        pl.when(c == 0)(lambda: transport(i))
        w_step(i + 2)
        pl.when(i == 1)(make_q)
        pl.when(i == 2)(place_q)
        pl.when(i == K + 2)(conv_gates)

        def one(r, _):
            j = jnp.where(r == 0, i - 2, i - 3)
            here = jnp.logical_and(j >= jnp.where(r == 2, 0, 1), j <= K)
            pl.when(here)(lambda: pair(j, r))
            return 0

        lax.fori_loop(0, 3, one, 0)
        return 0

    lax.fori_loop(1, K + 4, step, 0)

    for i in range(H):
        p, e = divmod(i, 2)
        theirs = slice(e * 2 * T + T, (e + 1) * 2 * T)
        o_send[i * VALUE : (i + 1) * VALUE, :] = o_acc[i][:, T:]
        o_send[H * VALUE + i : H * VALUE + i + 1, :] = m_acc[p][:, theirs]
        o_send[H * VALUE + H + i : H * VALUE + H + i + 1, :] = l_acc[p][:, theirs]
    o_exchange = remote(o_send, o_recv, o_s.at[0], o_r.at[0], partner)
    o_exchange.start()

    halo_copy(0, to_next).wait_recv()
    halo_copy(1, to_prev).wait_recv()
    g = gated[...]
    row = lax.broadcasted_iota(jnp.int32, g.shape, 0)
    before = jnp.where(sp == 0, 0.0, halo[0, 7:8, :])
    after = jnp.where(sp == SP - 1, 0.0, halo[1, 0:1, :])
    g_before = jnp.where(row == 0, before, pltpu.roll(g, 1, 0))
    g_after = jnp.where(row == T - 1, after, pltpu.roll(g, T - 1, 0))
    taps = conv_kernel[...].astype(F32)
    conv = g_before * taps[0:1] + g * taps[1:2] + g_after * taps[2:3]
    y_conv = (yconv[...] * conv).astype(BF16)

    o_exchange.wait_recv()
    parts = []
    for i in range(H):
        p, e = divmod(i, 2)
        ours = slice(e * 2 * T, e * 2 * T + T)
        m1 = m_acc[p][:, ours]
        m2 = o_recv[H * VALUE + i : H * VALUE + i + 1, :]
        top = jnp.maximum(m1, m2)
        a1, a2 = jnp.exp2(m1 - top), jnp.exp2(m2 - top)
        total = a1 * l_acc[p][:, ours] + a2 * o_recv[H * VALUE + H + i : H * VALUE + H + i + 1, :]
        summed = a1 * o_acc[i][:, :T] + a2 * o_recv[i * VALUE : (i + 1) * VALUE, :]
        parts.append(summed / total)
    y_attn = jnp.transpose(jnp.concatenate(parts, axis=0)).astype(BF16)
    y = jnp.concatenate([y_conv, y_attn], axis=1)
    for cp in out_cp:
        cp.wait()
    for rel, dev in ((2, to_xo), (1, to_xr), (3, to_xl), (0, None)):
        dest = lax.rem(x + rel, X)
        cols = pl.ds(pl.multiple_of(dest * DX, DX), DX)
        rs_send[rel] = dot_f32(y, wout[:, cols]).astype(BF16)
        if dev is not None:
            remote(rs_send.at[rel], rs_recv.at[rel - 1], r_s.at[rel - 1], r_r.at[rel - 1], dev).start()
    total = rs_send[0].astype(F32)
    r_copies = [
        remote(rs_send.at[rel], rs_recv.at[rel - 1], r_s.at[rel - 1], r_r.at[rel - 1], dev)
        for rel, dev in ((1, to_xr), (3, to_xl), (2, to_xo))
    ]
    for rel, cp in zip((1, 3, 2), r_copies):
        cp.wait_recv()
        total += rs_recv[rel - 1].astype(F32)
    out[...] = total.astype(BF16)

    for cp in tok_sends + [tok_copy(4, xl, lo, to_xr, False), tok_copy(5, xr, hi, to_xl, False)]:
        cp.wait_send()
    for cp in q_sends + [q_exchange, halo_copy(0, to_next), halo_copy(1, to_prev), o_exchange] + r_copies:
        cp.wait_send()

    w_own(c).wait_send()

    def w_sent(j, _):
        for core in (0, 1):
            for way in (0, 1):
                pl.when(j < K)(lambda way=way, core=core: w_far(z, j, way, core).wait_send())
                w_near(at(-STRIDE * j), way, core).wait_send()

            def back(core=core):
                w_near(at(STRIDE * j), 0, core).wait_send()
                pl.when(j < K)(lambda: w_near(at(STRIDE * j), 1, core).wait_send())

            pl.when(j >= 1)(back)
        return 0

    def w_handed(i, _):
        w_p(lax.rem(z + i, Z)).wait_send()
        return 0

    def w_all():
        lax.fori_loop(0, K + 1, w_sent, 0)
        lax.fori_loop(1, Z, w_handed, 0)

    pl.when(c == 1)(w_all)

    def k_sent(j, _):
        for way in (0, 1):
            pl.when(j < K)(lambda way=way: k_far(z, j, way).wait_send())
        k_near(at(-STRIDE * j), 0).wait_send()
        k_near(at(-STRIDE * j), 1).wait_send()

        def back():
            k_near(at(STRIDE * j), 0).wait_send()
            pl.when(j < K)(lambda: k_near(at(STRIDE * j), 1).wait_send())

        pl.when(j >= 1)(back)
        return 0

    def sent_slots(s, _):
        for kind, dev in ((0, to_xr), (1, to_xl), (2, to_xr)):
            k_x(s, x, kind, dev).wait_send()
        k_hand(s).wait_send()
        return 0

    def k_all():
        lax.fori_loop(0, K + 1, k_sent, 0)
        lax.fori_loop(0, Z, sent_slots, 0)

    pl.when(c == 0)(k_all)
    pl.when(c == 1)(k_own.wait_send)


def solution(mesh):
    SP, X = mesh.shape["sp"], mesh.shape["tp"]

    def per_device(
        tokens, mix_gain, wv, wo, wi, conv_kernel, wqd, wkvd, wrk, q_gain, kv_gain,
        wqn, wqr, wkn, wval, woc, woa,
    ):
        T, DX = tokens.shape
        D = DX * X
        Z = SP // 2
        R, CC = wv.shape
        H = wqn.shape[1] // NOPE
        nk, nq = wkvd.shape[1], wqd.shape[1]
        K = (Z // 2 - 1) // STRIDE
        RX = ROPE // X
        anyspace = pl.BlockSpec(memory_space=pl.ANY)
        vmem = pl.BlockSpec(memory_space=pltpu.VMEM)
        V = pltpu.VMEM
        DMA = pltpu.SemaphoreType.DMA
        scratch = [
            V((3, Z, 2, R, CC), BF16),
            V((X, T, DX), BF16),
            V((T, D), BF16),
            V(wqd.shape, BF16),
            V((128, D), BF16),
            V(wqn.shape, BF16), V(wqr.shape, BF16), V(wkn.shape, BF16), V(wval.shape, BF16),
            V((wval.shape[1], wval.shape[0]), BF16),
            V((woc.shape[0] + woa.shape[0], woc.shape[1]), BF16),
            V((X, nq, T), BF16),
            V((H * (NOPE + ROPE), T), BF16), V((H * (NOPE + ROPE), T), BF16),
            V((H // 2, 256, 4 * T), BF16),
            V((Z, X, 2, nk + 2 * RX, T), BF16), V((nk + 2 * RX, T), BF16),
            V((ROPE, T), F32), V((2, ROPE, T), F32),
            V((nq * X, 128), F32), V((nk * X, 128), F32),
            V((T, 128), F32),
            V((H, VALUE, 2 * T), F32), V((H // 2, 1, 4 * T), F32), V((H // 2, 1, 4 * T), F32),
            V((H * VALUE + 2 * H, T), F32), V((H * VALUE + 2 * H, T), F32),
            V((T, CC), F32), V((2, 8, CC), F32), V((T, CC), F32),
            V((X, T, DX), BF16), V((X - 1, T, DX), BF16),
            DMA((13,)),
            DMA((6,)), DMA((6,)),
            DMA((3,)), DMA((3,)), DMA((1,)), DMA((1,)),
            DMA((2, K)), DMA((Z, 2)), DMA((1,)), DMA((1,)), DMA((Z,)), DMA((Z,)), DMA((Z,)), DMA((Z, 3)), DMA((Z, 3)),
            DMA((2, K, 2)), DMA((Z, 2, 2)), DMA((Z, 2)), DMA((Z,)), DMA((Z,)), DMA((1,)), DMA((1,)),
            DMA((1,)), DMA((1,)), DMA((2,)), DMA((2,)), DMA((3,)), DMA((3,)),
        ]
        return pl.pallas_call(
            functools.partial(kernel, SP, X),
            out_shape=jax.ShapeDtypeStruct((T, DX), BF16),
            in_specs=[anyspace, vmem, anyspace, anyspace, anyspace, vmem, anyspace, anyspace, anyspace,
                      vmem, vmem] + [anyspace] * 6,
            out_specs=vmem,
            scratch_shapes=scratch,
            compiler_params=pltpu.CompilerParams(
                collective_id=0, has_side_effects=True, vmem_limit_bytes=56 * 1024 * 1024
            ),
        )(
            tokens, mix_gain.reshape(1, -1), wv, wo, wi, conv_kernel, wqd, wkvd.T, wrk.T,
            q_gain.reshape(1, -1), kv_gain.reshape(1, -1), wqn, wqr, wkn, wval, woc, woa,
        )

    placed = (
        P(("grp", "sp"), "tp"),
        P(),
        P("sp", "tp"),
        P("sp", "tp"),
        P("sp", "tp"),
        P(None, "tp"),
        P(None, "tp"),
        P(None, "tp"),
        P(),
        P(),
        P(),
        P(None, "tp"),
        P(None, "tp"),
        P(None, "tp"),
        P(None, "tp"),
        P("tp", None),
        P("tp", None),
    )
    return jax.shard_map(
        per_device, mesh=mesh, in_specs=placed, out_specs=P(("grp", "sp"), "tp"), check_vma=False
    )
```

```python
import functools
import math

import jax
import jax.numpy as jnp
from jax import lax
from jax.experimental import pallas as pl
from jax.experimental.pallas import tpu as pltpu
from jax.sharding import PartitionSpec as P

NOPE = 64
ROPE = 32
VALUE = 64
EPS = 1e-06
THETA = 10000.0
LOG2E = 1.4426950408889634
MESH = pl.DeviceIdType.MESH
F32 = jnp.float32
BF16 = jnp.bfloat16
STRIDE = 3
KC = 1
WC = 0


def dot_f32(a, b, contract=((1,), (0,))):
    return lax.dot_general(a, b, (contract, ((), ())), preferred_element_type=F32)


def kernel(
    SP, X,
    tokens, mix_gain, wv, wo, wi, conv_kernel, wqd, wkvd, wrk, q_gain, kv_gain,
    wqn, wqr, wkn, wval, woc, woa,
    out,
    wbuf, tok, scaled, wqd_v, wd_t, wqn_v, wqr_v, wkn_v, wval_v, wval_t, wout,
    qbuf, qmine, qpart, qz, kvbuf, kv_mine, rope_scr, cs_scr, qg_col, kvg_col, rs_scr,
    o_acc, m_acc, l_acc, o_send, o_recv, gated, halo, yconv, rs_send, rs_recv,
    loc, tk_s, tk_r, q_s, q_r, qp_s, qp_r, kf_s, kn_s, ko_s, ko_r, kh_s, kh_r, kz_r, kx_s, kx_r, wf_s, wn_s, wz_r, wp_s, wp_r, wq_s, wq_r,
    o_s, o_r, h_s, h_r, r_s, r_r,
):
    Z = SP // 2
    HALF = Z // 2
    K = (HALF - 1) // STRIDE
    assert HALF == STRIDE * K + 1
    T = tokens.shape[0]
    DX = tokens.shape[1]
    D = DX * X
    H = wqn.shape[1] // NOPE
    sp = lax.axis_index("sp")
    x = lax.axis_index("tp")
    z = lax.div(sp, 2)
    c = lax.rem(sp, 2)
    def core_at(step):
        return {"sp": lax.rem(z + step + Z, Z) * 2 + c}

    xr = lax.rem(x + 1, X)
    xl = lax.rem(x + X - 1, X)
    xo = lax.rem(x + 2, X)
    to_up, to_dn = core_at(1), core_at(-1)
    far_up, far_dn = core_at(STRIDE), core_at(-STRIDE)
    partner = {"sp": z * 2 + 1 - c}
    to_xr, to_xl, to_xo = {"tp": xr}, {"tp": xl}, {"tp": xo}
    prev_sp = lax.rem(sp + SP - 1, SP)
    next_sp = lax.rem(sp + 1, SP)
    other_chip = {"sp": jnp.where(c == 0, prev_sp, next_sp)}

    def remote(src, dst, ssem, rsem, dev):
        return pltpu.make_async_remote_copy(
            src_ref=src, dst_ref=dst, send_sem=ssem, recv_sem=rsem, device_id=dev, device_id_type=MESH
        )

    local = []
    def bring(src, dst):
        cp = pltpu.make_async_copy(src, dst, loc.at[len(local)])
        local.append(cp)
        cp.start()
        return cp

    conv_cp = [bring(w, wbuf.at[i, z, c]) for i, w in enumerate((wv, wo, wi))]
    tok_cp = bring(tokens, tok.at[x])
    nk, nr = wkvd.shape[0], wrk.shape[0]
    down_cp = [bring(wqd, wqd_v), bring(wkvd, wd_t.at[pl.ds(0, nk)]), bring(wrk, wd_t.at[pl.ds(nk, nr)])]
    up_cp = [bring(wqn, wqn_v), bring(wqr, wqr_v), bring(wkn, wkn_v), bring(wval, wval_v)]
    NC = woc.shape[0]
    out_cp = [bring(woc, wout.at[pl.ds(0, NC)]), bring(woa, wout.at[pl.ds(NC, woa.shape[0])])]

    barrier = pltpu.get_barrier_semaphore()
    for dev in (to_up, to_dn, far_up, far_dn, partner, to_xr, to_xl, to_xo, other_chip):
        pl.semaphore_signal(barrier, inc=1, device_id=dev, device_id_type=MESH)
    pl.semaphore_wait(barrier, 9)

    h = T // 2
    lo, hi = pl.ds(0, h), pl.ds(h, h)

    def tok_copy(k, piece, rows, dev, first):
        src = tokens.at[rows] if first else tok.at[piece, rows]
        return remote(src, tok.at[piece, rows], tk_s.at[k], tk_r.at[k], dev)

    tok_sends = [
        tok_copy(0, x, lo, to_xr, True), tok_copy(2, x, hi, to_xl, True),
        tok_copy(1, x, hi, to_xr, True), tok_copy(3, x, lo, to_xl, True),
    ]
    for cp in tok_sends:
        cp.start()

    def at(offset):
        return lax.rem(z + offset + 2 * Z, Z)

    def leaves(j, fn_up, fn_dn):
        def inner():
            fn_up(at(-STRIDE * j + 1))
            fn_dn(at(STRIDE * j - 1))

        fn_up(at(-STRIDE * j - 1))
        pl.when(j < K)(lambda: fn_dn(at(STRIDE * j + 1)))
        pl.when(j >= 1)(inner)

    def w_far(slot, j, way, core):
        piece = wbuf.at[:, slot, core]
        return remote(piece, piece, wf_s.at[way, j, core], wz_r.at[slot, core], far_dn if way else far_up)

    def w_near(slot, way, core):
        piece = wbuf.at[:, slot, core]
        return remote(piece, piece, wn_s.at[slot, way, core], wz_r.at[slot, core], to_dn if way else to_up)

    def w_p(slot):
        return remote(wbuf.at[:, slot], wbuf.at[:, slot], wp_s.at[slot], wp_r.at[slot], partner)

    def w_own(core):
        return remote(wbuf.at[:, z, core], wbuf.at[:, z, core], wq_s.at[0], wq_r.at[0], partner)

    for cp in conv_cp:
        cp.wait()
    w_own(c).start()

    def w_begin(core):
        for way in (0, 1):
            w_far(z, 0, way, core).start()
        for way in (0, 1):
            w_near(z, way, core).start()

    pl.when(c == WC)(lambda: w_begin(WC))

    def w_stop(j, way):
        slot = at(STRIDE * j if way else -STRIDE * j)
        for core in (WC, 1 - WC):
            w_near(slot, 0, core).wait_recv()
            pl.when(j < K)(lambda core=core: w_far(slot, j, way, core).start())

        def nears(to):
            for core in (WC, 1 - WC):
                w_near(slot, to, core).start()

        nears(0)
        if way == 0:
            nears(1)
        else:
            pl.when(j < K)(lambda: nears(1))
        w_p(slot).start()

    def w_leaf(slot):
        for core in (WC, 1 - WC):
            w_near(slot, 0, core).wait_recv()
        w_p(slot).start()

    def w_step(j):
        def stops_in():
            w_stop(j, 0)
            w_stop(j, 1)

        pl.when(jnp.logical_and(c == WC, j <= K))(stops_in)
        pl.when(jnp.logical_and(c == WC, j <= K + 1))(lambda: leaves(j - 1, w_leaf, w_leaf))

    wd_t[nk + nr :, :] = jnp.zeros((wd_t.shape[0] - nk - nr, D), BF16)
    rows16 = lax.broadcasted_iota(jnp.int32, (ROPE, T), 0)
    freq = jnp.where(rows16 >= ROPE // 2, rows16 - ROPE // 2, rows16).astype(F32) * 2.0
    inverse = jnp.exp(freq * (-math.log(THETA) / ROPE))
    phase = (sp * T + lax.broadcasted_iota(jnp.int32, (ROPE, T), 1)).astype(F32) * inverse
    cs_scr[0] = jnp.cos(phase)
    cs_scr[1] = jnp.sin(phase)
    qg_col[...] = jnp.transpose(jnp.broadcast_to(q_gain[...].astype(F32), (128, q_gain.shape[1])))
    kvg_col[...] = jnp.transpose(jnp.broadcast_to(kv_gain[...].astype(F32), (128, kv_gain.shape[1])))
    qz[...] = jnp.zeros(qz.shape, BF16)
    o_acc[...] = jnp.zeros(o_acc.shape, F32)
    m_acc[...] = jnp.full(m_acc.shape, -jnp.inf, F32)
    l_acc[...] = jnp.zeros(l_acc.shape, F32)
    for cp in up_cp:
        cp.wait()
    wval_t[...] = jnp.transpose(wval_v[...].astype(F32)).astype(BF16)

    w_own(1 - c).wait_recv()
    pl.when(c == WC)(lambda: w_begin(1 - WC))
    tok_copy(0, xl, lo, to_xr, False).wait_recv()
    tok_copy(4, xl, lo, to_xr, False).start()
    tok_copy(2, xr, hi, to_xl, False).wait_recv()
    tok_copy(5, xr, hi, to_xl, False).start()
    tok_copy(1, xl, hi, to_xr, False).wait_recv()
    tok_copy(3, xr, lo, to_xl, False).wait_recv()
    w_step(1)
    tok_copy(4, xo, lo, to_xr, False).wait_recv()
    tok_copy(5, xo, hi, to_xl, False).wait_recv()
    tok_cp.wait()

    for cp in down_cp:
        cp.wait()
    down_q = jnp.zeros((T, wqd.shape[1]), F32)
    down_k = jnp.zeros((T, wd_t.shape[0]), F32)
    squares = jnp.zeros((T, 1), F32)
    for j in range(X):
        t = tok[j].astype(F32)
        s = (t * mix_gain[:, j * DX : (j + 1) * DX].astype(F32)).astype(BF16)
        scaled[:, j * DX : (j + 1) * DX] = s
        squares += jnp.sum(t * t, axis=1, keepdims=True)
        down_q += dot_f32(s, wqd_v[j * DX : (j + 1) * DX, :])
        down_k += dot_f32(s, wd_t[:, j * DX : (j + 1) * DX], ((1,), (1,)))
    row_scale = lax.rsqrt(squares / D + EPS)
    rs_scr[...] = jnp.broadcast_to(row_scale, rs_scr.shape)
    down_t = jnp.transpose(jnp.concatenate([down_q, down_k], axis=1) * row_scale)
    nq = wqd.shape[1]
    kv_mine[:nk, :] = down_t[nq : nq + nk].astype(BF16)

    def turned(v, cosine, sine):
        half = ROPE // 2
        return v * cosine + jnp.concatenate([-v[half:], v[:half]], axis=0) * sine

    raw = down_t[nq + nk : nq + nk + nr].astype(BF16).astype(F32)
    rope_scr[...] = turned(raw, cs_scr[0], cs_scr[1])
    RX = ROPE // X
    mine = rope_scr[pl.ds(pl.multiple_of(x * RX, RX), RX), :]
    kv_mine[nk:, :] = jnp.concatenate([mine, jnp.zeros((RX, T), F32)], axis=0).astype(BF16)
    k_own = remote(kv_mine, kvbuf.at[z, x, 1 - KC], ko_s.at[0], ko_r.at[0], partner)
    pl.when(c != KC)(k_own.start)

    def keep_mine():
        kvbuf[z, x, KC] = kv_mine[...]

    pl.when(c == KC)(keep_mine)

    def k_far(slot, j, way):
        piece = kvbuf.at[slot, x]
        return remote(piece, piece, kf_s.at[way, j], kz_r.at[slot], far_dn if way else far_up)

    def k_near(slot, way):
        piece = kvbuf.at[slot, x]
        return remote(piece, piece, kn_s.at[slot, way], kz_r.at[slot], to_dn if way else to_up)

    def k_x(slot, piece, kind, dev):
        return remote(kvbuf.at[slot, piece], kvbuf.at[slot, piece], kx_s.at[slot, kind], kx_r.at[slot, kind], dev)

    def k_hand(slot):
        return remote(kvbuf.at[slot, :, 1 - KC], kvbuf.at[slot, :, 1 - KC], kh_s.at[slot], kh_r.at[slot], partner)

    def k_begin():
        k_own.wait_recv()
        k_far(z, 0, 0).start()
        k_far(z, 0, 1).start()
        k_near(z, 0).start()
        k_near(z, 1).start()
        k_x(z, x, 0, to_xr).start()
        k_x(z, x, 1, to_xl).start()


    qbuf[x] = down_t[:nq].astype(BF16)

    def q_copy(kind, piece, dev):
        return remote(qbuf.at[piece], qbuf.at[piece], q_s.at[kind], q_r.at[kind], dev)

    q_sends = [q_copy(2, x, to_xo), q_copy(0, x, to_xr), q_copy(1, x, to_xl)]
    for cp in q_sends:
        cp.start()
    pl.when(c == KC)(k_begin)
    w_step(2)

    factor = (NOPE + ROPE) ** (-0.5) * LOG2E
    q_exchange = remote(qmine, qpart, qp_s.at[0], qp_r.at[0], partner)

    def make_q():
        q_copy(0, xl, to_xr).wait_recv()
        q_copy(1, xr, to_xl).wait_recv()
        q_copy(2, xo, to_xo).wait_recv()
        qf = qbuf[...].reshape(X * nq, T).astype(F32)
        scale = lax.rsqrt(jnp.mean(qf * qf, axis=0, keepdims=True) + EPS)
        qn = (qf * scale * qg_col[...]).astype(BF16)
        nope = dot_f32(wqn_v[...], qn, ((0,), (0,))) * factor
        qmine[: H * NOPE, :] = nope.astype(BF16)
        rope = dot_f32(wqr_v[...], qn, ((0,), (0,)))
        for i in range(H):
            r = turned(rope[i * ROPE : (i + 1) * ROPE], cs_scr[0], cs_scr[1]) * factor
            qmine[H * NOPE + i * ROPE : H * NOPE + (i + 1) * ROPE, :] = r.astype(BF16)
        q_exchange.start()

    def place_q():
        q_exchange.wait_recv()
        for i in range(H):
            p, e = divmod(i, 2)
            for src, at in ((qmine, 0), (qpart, T)):
                cols = slice(e * 2 * T + at, e * 2 * T + at + T)
                qz[p, e * NOPE : (e + 1) * NOPE, cols] = src[i * NOPE : (i + 1) * NOPE, :]
                qz[p, 2 * NOPE : 2 * NOPE + ROPE, cols] = src[H * NOPE + i * ROPE : H * NOPE + (i + 1) * ROPE, :]

    def keys(slot):
        lat = kvbuf[slot, :, c, :nk, :].reshape(X * nk, T).astype(F32)
        rope = kvbuf[slot, :, c, nk : nk + 2 * RX, :].astype(F32)[:, :RX].reshape(ROPE, T)
        return lat, rope

    def chunk(slot_a, slot_b):
        la, ra = keys(slot_a)
        lb, rb = keys(slot_b)
        lat = jnp.concatenate([la, lb], axis=1)
        scale = lax.rsqrt(jnp.mean(lat * lat, axis=0, keepdims=True) + EPS)
        gain = kvg_col[...]
        n = (lat * scale * jnp.concatenate([gain, gain], axis=1)).astype(BF16)
        kn = dot_f32(n, wkn_v[...], ((0,), (0,))).astype(BF16)
        rope = jnp.concatenate([ra, rb], axis=1)
        kr = jnp.transpose(jnp.concatenate([rope, jnp.zeros((128 - ROPE, 2 * T), F32)], axis=0)).astype(BF16)
        vt = dot_f32(wval_t[...], n).astype(BF16)
        for p in range(H // 2):
            kp = jnp.concatenate([kn[:, p * 128 : (p + 1) * 128], kr], axis=1)
            s = dot_f32(kp, qz[p])
            old = m_acc[p]
            new = jnp.maximum(old, jnp.max(s, axis=0, keepdims=True))
            m_acc[p] = new
            fade = jnp.exp2(old - new)
            w = jnp.exp2(s - new)
            l_acc[p] = l_acc[p] * fade + jnp.sum(w, axis=0, keepdims=True)
            wb = w.astype(BF16)
            for e in range(2):
                i = 2 * p + e
                cols = slice(e * 2 * T, (e + 1) * 2 * T)
                o_acc[i] = o_acc[i] * fade[:, cols] + dot_f32(vt[i * VALUE : (i + 1) * VALUE], wb[:, cols])

    def halo_copy(k, dev):
        rows = pl.ds(0, 8) if k == 1 else pl.ds(T - 8, 8)
        return remote(gated.at[rows], halo.at[k], h_s.at[k], h_r.at[k], dev)

    to_next, to_prev = {"sp": next_sp}, {"sp": prev_sp}

    def conv_gates():
        def got(i, _):
            w_p(lax.rem(z + i, Z)).wait_recv()
            return 0

        def all_in():
            lax.fori_loop(1, Z, got, 0)

        pl.when(c != WC)(all_in)

        def project(i):
            w = wbuf[i].reshape(D, wbuf.shape[-1])
            return (dot_f32(scaled[...], w) * rs_scr[:, 0:1]).astype(BF16).astype(F32)
        inner = project(2)
        value = project(0)
        gated[...] = (inner * value).astype(BF16).astype(F32)
        halo_copy(0, to_next).start()
        halo_copy(1, to_prev).start()
        yconv[...] = project(1)

    def spread(slot):
        k_x(slot, x, 0, to_xr).start()
        k_x(slot, x, 1, to_xl).start()

    def stop(j, way):
        slot = at(STRIDE * j if way else -STRIDE * j)
        k_near(slot, 0).wait_recv()
        pl.when(j < K)(lambda: k_far(slot, j, way).start())
        if way == 0:
            k_near(slot, 0).start()
            k_near(slot, 1).start()
        else:
            k_near(slot, 0).start()
            pl.when(j < K)(lambda: k_near(slot, 1).start())
        spread(slot)

    def leaf(slot):
        k_near(slot, 0).wait_recv()
        spread(slot)

    def relay_up(slot):
        k_x(slot, xl, 0, to_xr).wait_recv()
        k_x(slot, xl, 2, to_xr).start()

    def relay_dn(slot):
        k_x(slot, xr, 1, to_xl).wait_recv()
        k_x(slot, xr, 2, to_xl).start()

    def got_up(slot):
        k_x(slot, xr, 1, to_xl).wait_recv()
        k_x(slot, xo, 2, to_xr).wait_recv()

    def got_dn(slot):
        k_x(slot, xl, 0, to_xr).wait_recv()
        k_x(slot, xo, 2, to_xl).wait_recv()

    def pair(j, r):
        off = STRIDE * j + jnp.where(r == 0, 0, jnp.where(r == 1, -1, 1))
        own = off == HALF
        slot_a = at(-off)
        slot_b = jnp.where(own, z, at(off))

        def take():
            got_up(slot_a)
            pl.when(own)(lambda: got_up(slot_b))
            pl.when(jnp.logical_not(own))(lambda: got_dn(slot_b))
            k_hand(slot_a).start()
            k_hand(slot_b).start()

        def handed():
            k_hand(slot_a).wait_recv()
            k_hand(slot_b).wait_recv()

        pl.when(c == KC)(take)
        pl.when(c != KC)(handed)
        chunk(slot_a, slot_b)

    def transport(i):
        def stops_in():
            stop(i, 0)
            stop(i, 1)

        pl.when(i <= K)(stops_in)
        pl.when(i - 1 <= K)(lambda: leaves(i - 1, leaf, leaf))

        def relay_stops():
            relay_up(at(-STRIDE * (i - 1)))
            pl.when(i - 1 >= 1)(lambda: relay_dn(at(STRIDE * (i - 1))))

        pl.when(i - 1 <= K)(relay_stops)
        pl.when(jnp.logical_and(i - 2 >= 0, i - 2 <= K))(lambda: leaves(i - 2, relay_up, relay_dn))

    def step(i, _):
        pl.when(c == KC)(lambda: transport(i))
        w_step(i + 2)
        pl.when(i == 1)(make_q)
        pl.when(i == 2)(place_q)
        pl.when(i == K + 2)(conv_gates)

        def one(r, _):
            j = jnp.where(r == 0, i - 2, i - 3)
            here = jnp.logical_and(j >= jnp.where(r == 2, 0, 1), j <= K)
            pl.when(here)(lambda: pair(j, r))
            return 0

        lax.fori_loop(0, 3, one, 0)
        return 0

    lax.fori_loop(1, K + 4, step, 0)

    for i in range(H):
        p, e = divmod(i, 2)
        theirs = slice(e * 2 * T + T, (e + 1) * 2 * T)
        o_send[i * VALUE : (i + 1) * VALUE, :] = o_acc[i][:, T:]
        o_send[H * VALUE + i : H * VALUE + i + 1, :] = m_acc[p][:, theirs]
        o_send[H * VALUE + H + i : H * VALUE + H + i + 1, :] = l_acc[p][:, theirs]
    o_exchange = remote(o_send, o_recv, o_s.at[0], o_r.at[0], partner)
    o_exchange.start()

    halo_copy(0, to_next).wait_recv()
    halo_copy(1, to_prev).wait_recv()
    g = gated[...]
    row = lax.broadcasted_iota(jnp.int32, g.shape, 0)
    before = jnp.where(sp == 0, 0.0, halo[0, 7:8, :])
    after = jnp.where(sp == SP - 1, 0.0, halo[1, 0:1, :])
    g_before = jnp.where(row == 0, before, pltpu.roll(g, 1, 0))
    g_after = jnp.where(row == T - 1, after, pltpu.roll(g, T - 1, 0))
    taps = conv_kernel[...].astype(F32)
    conv = g_before * taps[0:1] + g * taps[1:2] + g_after * taps[2:3]
    y_conv = (yconv[...] * conv).astype(BF16)

    o_exchange.wait_recv()
    parts = []
    for i in range(H):
        p, e = divmod(i, 2)
        ours = slice(e * 2 * T, e * 2 * T + T)
        m1 = m_acc[p][:, ours]
        m2 = o_recv[H * VALUE + i : H * VALUE + i + 1, :]
        top = jnp.maximum(m1, m2)
        a1, a2 = jnp.exp2(m1 - top), jnp.exp2(m2 - top)
        total = a1 * l_acc[p][:, ours] + a2 * o_recv[H * VALUE + H + i : H * VALUE + H + i + 1, :]
        summed = a1 * o_acc[i][:, :T] + a2 * o_recv[i * VALUE : (i + 1) * VALUE, :]
        parts.append(summed / total)
    y_attn = jnp.transpose(jnp.concatenate(parts, axis=0)).astype(BF16)
    y = jnp.concatenate([y_conv, y_attn], axis=1)
    for cp in out_cp:
        cp.wait()
    for rel, dev in ((2, to_xo), (1, to_xr), (3, to_xl), (0, None)):
        dest = lax.rem(x + rel, X)
        cols = pl.ds(pl.multiple_of(dest * DX, DX), DX)
        rs_send[rel] = dot_f32(y, wout[:, cols]).astype(BF16)
        if dev is not None:
            remote(rs_send.at[rel], rs_recv.at[rel - 1], r_s.at[rel - 1], r_r.at[rel - 1], dev).start()
    for cp in tok_sends + [tok_copy(4, xl, lo, to_xr, False), tok_copy(5, xr, hi, to_xl, False)]:
        cp.wait_send()
    for cp in q_sends + [q_exchange, halo_copy(0, to_next), halo_copy(1, to_prev), o_exchange]:
        cp.wait_send()

    w_own(c).wait_send()

    def w_sent(j, _):
        for core in (0, 1):
            for way in (0, 1):
                pl.when(j < K)(lambda way=way, core=core: w_far(z, j, way, core).wait_send())
                w_near(at(-STRIDE * j), way, core).wait_send()

            def back(core=core):
                w_near(at(STRIDE * j), 0, core).wait_send()
                pl.when(j < K)(lambda: w_near(at(STRIDE * j), 1, core).wait_send())

            pl.when(j >= 1)(back)
        return 0

    def w_handed(i, _):
        w_p(lax.rem(z + i, Z)).wait_send()
        return 0

    def w_all():
        lax.fori_loop(0, K + 1, w_sent, 0)
        lax.fori_loop(1, Z, w_handed, 0)

    pl.when(c == WC)(w_all)

    def k_sent(j, _):
        for way in (0, 1):
            pl.when(j < K)(lambda way=way: k_far(z, j, way).wait_send())
        k_near(at(-STRIDE * j), 0).wait_send()
        k_near(at(-STRIDE * j), 1).wait_send()

        def back():
            k_near(at(STRIDE * j), 0).wait_send()
            pl.when(j < K)(lambda: k_near(at(STRIDE * j), 1).wait_send())

        pl.when(j >= 1)(back)
        return 0

    def sent_slots(s, _):
        for kind, dev in ((0, to_xr), (1, to_xl), (2, to_xr)):
            k_x(s, x, kind, dev).wait_send()
        k_hand(s).wait_send()
        return 0

    def k_all():
        lax.fori_loop(0, K + 1, k_sent, 0)
        lax.fori_loop(0, Z, sent_slots, 0)

    pl.when(c == KC)(k_all)
    pl.when(c != KC)(k_own.wait_send)

    total = rs_send[0].astype(F32)
    r_copies = [
        remote(rs_send.at[rel], rs_recv.at[rel - 1], r_s.at[rel - 1], r_r.at[rel - 1], dev)
        for rel, dev in ((1, to_xr), (3, to_xl), (2, to_xo))
    ]
    for rel, cp in zip((1, 3, 2), r_copies):
        cp.wait_recv()
        total += rs_recv[rel - 1].astype(F32)
    out[...] = total.astype(BF16)
    for cp in r_copies:
        cp.wait_send()


def solution(mesh):
    SP, X = mesh.shape["sp"], mesh.shape["tp"]

    def per_device(
        tokens, mix_gain, wv, wo, wi, conv_kernel, wqd, wkvd, wrk, q_gain, kv_gain,
        wqn, wqr, wkn, wval, woc, woa,
    ):
        T, DX = tokens.shape
        D = DX * X
        Z = SP // 2
        R, CC = wv.shape
        H = wqn.shape[1] // NOPE
        nk, nq = wkvd.shape[1], wqd.shape[1]
        K = (Z // 2 - 1) // STRIDE
        RX = ROPE // X
        anyspace = pl.BlockSpec(memory_space=pl.ANY)
        vmem = pl.BlockSpec(memory_space=pltpu.VMEM)
        V = pltpu.VMEM
        DMA = pltpu.SemaphoreType.DMA
        scratch = [
            V((3, Z, 2, R, CC), BF16),
            V((X, T, DX), BF16),
            V((T, D), BF16),
            V(wqd.shape, BF16),
            V((128, D), BF16),
            V(wqn.shape, BF16), V(wqr.shape, BF16), V(wkn.shape, BF16), V(wval.shape, BF16),
            V((wval.shape[1], wval.shape[0]), BF16),
            V((woc.shape[0] + woa.shape[0], woc.shape[1]), BF16),
            V((X, nq, T), BF16),
            V((H * (NOPE + ROPE), T), BF16), V((H * (NOPE + ROPE), T), BF16),
            V((H // 2, 256, 4 * T), BF16),
            V((Z, X, 2, nk + 2 * RX, T), BF16), V((nk + 2 * RX, T), BF16),
            V((ROPE, T), F32), V((2, ROPE, T), F32),
            V((nq * X, 128), F32), V((nk * X, 128), F32),
            V((T, 128), F32),
            V((H, VALUE, 2 * T), F32), V((H // 2, 1, 4 * T), F32), V((H // 2, 1, 4 * T), F32),
            V((H * VALUE + 2 * H, T), F32), V((H * VALUE + 2 * H, T), F32),
            V((T, CC), F32), V((2, 8, CC), F32), V((T, CC), F32),
            V((X, T, DX), BF16), V((X - 1, T, DX), BF16),
            DMA((13,)),
            DMA((6,)), DMA((6,)),
            DMA((3,)), DMA((3,)), DMA((1,)), DMA((1,)),
            DMA((2, K)), DMA((Z, 2)), DMA((1,)), DMA((1,)), DMA((Z,)), DMA((Z,)), DMA((Z,)), DMA((Z, 3)), DMA((Z, 3)),
            DMA((2, K, 2)), DMA((Z, 2, 2)), DMA((Z, 2)), DMA((Z,)), DMA((Z,)), DMA((1,)), DMA((1,)),
            DMA((1,)), DMA((1,)), DMA((2,)), DMA((2,)), DMA((3,)), DMA((3,)),
        ]
        return pl.pallas_call(
            functools.partial(kernel, SP, X),
            out_shape=jax.ShapeDtypeStruct((T, DX), BF16),
            in_specs=[anyspace, vmem, anyspace, anyspace, anyspace, vmem, anyspace, anyspace, anyspace,
                      vmem, vmem] + [anyspace] * 6,
            out_specs=vmem,
            scratch_shapes=scratch,
            compiler_params=pltpu.CompilerParams(
                collective_id=0, has_side_effects=True, vmem_limit_bytes=56 * 1024 * 1024
            ),
        )(
            tokens, mix_gain.reshape(1, -1), wv, wo, wi, conv_kernel, wqd, wkvd.T, wrk.T,
            q_gain.reshape(1, -1), kv_gain.reshape(1, -1), wqn, wqr, wkn, wval, woc, woa,
        )

    placed = (
        P(("grp", "sp"), "tp"),
        P(),
        P("sp", "tp"),
        P("sp", "tp"),
        P("sp", "tp"),
        P(None, "tp"),
        P(None, "tp"),
        P(None, "tp"),
        P(),
        P(),
        P(),
        P(None, "tp"),
        P(None, "tp"),
        P(None, "tp"),
        P(None, "tp"),
        P("tp", None),
        P("tp", None),
    )
    return jax.shard_map(
        per_device, mesh=mesh, in_specs=placed, out_specs=P(("grp", "sp"), "tp"), check_vma=False
    )
```

```python
import functools
import math

import jax
import jax.numpy as jnp
from jax import lax
from jax.experimental import pallas as pl
from jax.experimental.pallas import tpu as pltpu
from jax.sharding import PartitionSpec as P

NOPE = 64
ROPE = 32
VALUE = 64
EPS = 1e-06
THETA = 10000.0
LOG2E = 1.4426950408889634
MESH = pl.DeviceIdType.MESH
F32 = jnp.float32
BF16 = jnp.bfloat16
STRIDE = 3
KC = 0
WC = 1


def dot_f32(a, b, contract=((1,), (0,))):
    return lax.dot_general(a, b, (contract, ((), ())), preferred_element_type=F32)


def kernel(
    SP, X,
    tokens, mix_gain, wv, wo, wi, conv_kernel, wqd, wkvd, wrk, q_gain, kv_gain,
    wqn, wqr, wkn, wval, woc, woa,
    out,
    wbuf, tok, scaled, wqd_v, wd_t, wqn_v, wqr_v, wkn_v, wval_v, wval_t, wout,
    qbuf, qmine, qpart, qz, kvbuf, kv_mine, rope_scr, cs_scr, qg_col, kvg_col, rs_scr,
    o_acc, m_acc, l_acc, o_send, o_recv, gated, halo, yconv, rs_send, rs_recv,
    loc, tk_s, tk_r, q_s, q_r, qp_s, qp_r, kf_s, kn_s, ko_s, ko_r, kh_s, kh_r, kz_r, kx_s, kx_r, wf_s, wn_s, wz_r, wp_s, wp_r, wq_s, wq_r,
    o_s, o_r, h_s, h_r, r_s, r_r,
):
    Z = SP // 2
    HALF = Z // 2
    K = (HALF - 1) // STRIDE
    assert HALF == STRIDE * K + 1
    T = tokens.shape[0]
    DX = tokens.shape[1]
    D = DX * X
    H = wqn.shape[1] // NOPE
    sp = lax.axis_index("sp")
    x = lax.axis_index("tp")
    z = lax.div(sp, 2)
    c = lax.rem(sp, 2)
    def core_at(step):
        return {"sp": lax.rem(z + step + Z, Z) * 2 + c}

    xr = lax.rem(x + 1, X)
    xl = lax.rem(x + X - 1, X)
    xo = lax.rem(x + 2, X)
    to_up, to_dn = core_at(1), core_at(-1)
    far_up, far_dn = core_at(STRIDE), core_at(-STRIDE)
    partner = {"sp": z * 2 + 1 - c}
    to_xr, to_xl, to_xo = {"tp": xr}, {"tp": xl}, {"tp": xo}
    prev_sp = lax.rem(sp + SP - 1, SP)
    next_sp = lax.rem(sp + 1, SP)
    other_chip = {"sp": jnp.where(c == 0, prev_sp, next_sp)}

    def remote(src, dst, ssem, rsem, dev):
        return pltpu.make_async_remote_copy(
            src_ref=src, dst_ref=dst, send_sem=ssem, recv_sem=rsem, device_id=dev, device_id_type=MESH
        )

    local = []
    def bring(src, dst):
        cp = pltpu.make_async_copy(src, dst, loc.at[len(local)])
        local.append(cp)
        cp.start()
        return cp

    conv_cp = [bring(w, wbuf.at[i, z, c]) for i, w in enumerate((wv, wo, wi))]
    tok_cp = bring(tokens, tok.at[x])
    nk, nr = wkvd.shape[0], wrk.shape[0]
    down_cp = [bring(wqd, wqd_v), bring(wkvd, wd_t.at[pl.ds(0, nk)]), bring(wrk, wd_t.at[pl.ds(nk, nr)])]
    up_cp = [bring(wqn, wqn_v), bring(wqr, wqr_v), bring(wkn, wkn_v), bring(wval, wval_v)]
    NC = woc.shape[0]
    out_cp = [bring(woc, wout.at[pl.ds(0, NC)]), bring(woa, wout.at[pl.ds(NC, woa.shape[0])])]

    barrier = pltpu.get_barrier_semaphore()
    for dev in (to_up, to_dn, far_up, far_dn, partner, to_xr, to_xl, to_xo, other_chip):
        pl.semaphore_signal(barrier, inc=1, device_id=dev, device_id_type=MESH)
    pl.semaphore_wait(barrier, 9)

    h = T // 2
    lo, hi = pl.ds(0, h), pl.ds(h, h)

    def tok_copy(k, piece, rows, dev, first):
        src = tokens.at[rows] if first else tok.at[piece, rows]
        return remote(src, tok.at[piece, rows], tk_s.at[k], tk_r.at[k], dev)

    tok_sends = [
        tok_copy(0, x, lo, to_xr, True), tok_copy(2, x, hi, to_xl, True),
        tok_copy(1, x, hi, to_xr, True), tok_copy(3, x, lo, to_xl, True),
    ]
    for cp in tok_sends:
        cp.start()

    def at(offset):
        return lax.rem(z + offset + 2 * Z, Z)

    def leaves(j, fn_up, fn_dn):
        def inner():
            fn_up(at(-STRIDE * j + 1))
            fn_dn(at(STRIDE * j - 1))

        fn_up(at(-STRIDE * j - 1))
        pl.when(j < K)(lambda: fn_dn(at(STRIDE * j + 1)))
        pl.when(j >= 1)(inner)

    def w_far(slot, j, way, core):
        piece = wbuf.at[:, slot, core]
        return remote(piece, piece, wf_s.at[way, j, core], wz_r.at[slot, core], far_dn if way else far_up)

    def w_near(slot, way, core):
        piece = wbuf.at[:, slot, core]
        return remote(piece, piece, wn_s.at[slot, way, core], wz_r.at[slot, core], to_dn if way else to_up)

    def w_p(slot):
        return remote(wbuf.at[:, slot], wbuf.at[:, slot], wp_s.at[slot], wp_r.at[slot], partner)

    def w_own(core):
        return remote(wbuf.at[:, z, core], wbuf.at[:, z, core], wq_s.at[0], wq_r.at[0], partner)

    for cp in conv_cp:
        cp.wait()
    w_own(c).start()

    def w_begin(core):
        for way in (0, 1):
            w_far(z, 0, way, core).start()
        for way in (0, 1):
            w_near(z, way, core).start()

    pl.when(c == WC)(lambda: w_begin(WC))

    def w_stop(j, way):
        slot = at(STRIDE * j if way else -STRIDE * j)
        for core in (WC, 1 - WC):
            w_near(slot, 0, core).wait_recv()
            pl.when(j < K)(lambda core=core: w_far(slot, j, way, core).start())

        def nears(to):
            for core in (WC, 1 - WC):
                w_near(slot, to, core).start()

        nears(0)
        if way == 0:
            nears(1)
        else:
            pl.when(j < K)(lambda: nears(1))
        w_p(slot).start()

    def w_leaf(slot):
        for core in (WC, 1 - WC):
            w_near(slot, 0, core).wait_recv()
        w_p(slot).start()

    def w_step(j):
        def stops_in():
            w_stop(j, 0)
            w_stop(j, 1)

        pl.when(jnp.logical_and(c == WC, j <= K))(stops_in)
        pl.when(jnp.logical_and(c == WC, j <= K + 1))(lambda: leaves(j - 1, w_leaf, w_leaf))

    wd_t[nk + nr :, :] = jnp.zeros((wd_t.shape[0] - nk - nr, D), BF16)
    rows16 = lax.broadcasted_iota(jnp.int32, (ROPE, T), 0)
    freq = jnp.where(rows16 >= ROPE // 2, rows16 - ROPE // 2, rows16).astype(F32) * 2.0
    inverse = jnp.exp(freq * (-math.log(THETA) / ROPE))
    phase = (sp * T + lax.broadcasted_iota(jnp.int32, (ROPE, T), 1)).astype(F32) * inverse
    cs_scr[0] = jnp.cos(phase)
    cs_scr[1] = jnp.sin(phase)
    qg_col[...] = jnp.transpose(jnp.broadcast_to(q_gain[...].astype(F32), (128, q_gain.shape[1])))
    kvg_col[...] = jnp.transpose(jnp.broadcast_to(kv_gain[...].astype(F32), (128, kv_gain.shape[1])))
    qz[...] = jnp.zeros(qz.shape, BF16)
    o_acc[...] = jnp.zeros(o_acc.shape, F32)
    m_acc[...] = jnp.full(m_acc.shape, -jnp.inf, F32)
    l_acc[...] = jnp.zeros(l_acc.shape, F32)
    for cp in up_cp:
        cp.wait()
    wval_t[...] = jnp.transpose(wval_v[...].astype(F32)).astype(BF16)

    w_own(1 - c).wait_recv()
    pl.when(c == WC)(lambda: w_begin(1 - WC))
    tok_copy(0, xl, lo, to_xr, False).wait_recv()
    tok_copy(4, xl, lo, to_xr, False).start()
    tok_copy(2, xr, hi, to_xl, False).wait_recv()
    tok_copy(5, xr, hi, to_xl, False).start()
    tok_copy(1, xl, hi, to_xr, False).wait_recv()
    tok_copy(3, xr, lo, to_xl, False).wait_recv()
    w_step(1)
    tok_copy(4, xo, lo, to_xr, False).wait_recv()
    tok_copy(5, xo, hi, to_xl, False).wait_recv()
    tok_cp.wait()

    for cp in down_cp:
        cp.wait()
    down_q = jnp.zeros((T, wqd.shape[1]), F32)
    down_k = jnp.zeros((T, wd_t.shape[0]), F32)
    squares = jnp.zeros((T, 1), F32)
    for j in range(X):
        t = tok[j].astype(F32)
        s = (t * mix_gain[:, j * DX : (j + 1) * DX].astype(F32)).astype(BF16)
        scaled[:, j * DX : (j + 1) * DX] = s
        squares += jnp.sum(t * t, axis=1, keepdims=True)
        down_q += dot_f32(s, wqd_v[j * DX : (j + 1) * DX, :])
        down_k += dot_f32(s, wd_t[:, j * DX : (j + 1) * DX], ((1,), (1,)))
    row_scale = lax.rsqrt(squares / D + EPS)
    rs_scr[...] = jnp.broadcast_to(row_scale, rs_scr.shape)
    down_t = jnp.transpose(jnp.concatenate([down_q, down_k], axis=1) * row_scale)
    nq = wqd.shape[1]
    kv_mine[:nk, :] = down_t[nq : nq + nk].astype(BF16)

    def turned(v, cosine, sine):
        half = ROPE // 2
        return v * cosine + jnp.concatenate([-v[half:], v[:half]], axis=0) * sine

    raw = down_t[nq + nk : nq + nk + nr].astype(BF16).astype(F32)
    rope_scr[...] = turned(raw, cs_scr[0], cs_scr[1])
    RX = ROPE // X
    mine = rope_scr[pl.ds(pl.multiple_of(x * RX, RX), RX), :]
    kv_mine[nk:, :] = jnp.concatenate([mine, jnp.zeros((RX, T), F32)], axis=0).astype(BF16)
    k_own = remote(kv_mine, kvbuf.at[z, x, 1 - KC], ko_s.at[0], ko_r.at[0], partner)
    pl.when(c != KC)(k_own.start)

    def keep_mine():
        kvbuf[z, x, KC] = kv_mine[...]

    pl.when(c == KC)(keep_mine)

    def k_far(slot, j, way):
        piece = kvbuf.at[slot, x]
        return remote(piece, piece, kf_s.at[way, j], kz_r.at[slot], far_dn if way else far_up)

    def k_near(slot, way):
        piece = kvbuf.at[slot, x]
        return remote(piece, piece, kn_s.at[slot, way], kz_r.at[slot], to_dn if way else to_up)

    def k_x(slot, piece, kind, dev):
        return remote(kvbuf.at[slot, piece], kvbuf.at[slot, piece], kx_s.at[slot, kind], kx_r.at[slot, kind], dev)

    def k_hand(slot):
        return remote(kvbuf.at[slot, :, 1 - KC], kvbuf.at[slot, :, 1 - KC], kh_s.at[slot], kh_r.at[slot], partner)

    def k_begin():
        k_own.wait_recv()
        k_far(z, 0, 0).start()
        k_far(z, 0, 1).start()
        k_near(z, 0).start()
        k_near(z, 1).start()
        k_x(z, x, 0, to_xr).start()
        k_x(z, x, 1, to_xl).start()


    qbuf[x] = down_t[:nq].astype(BF16)

    def q_copy(kind, piece, dev):
        return remote(qbuf.at[piece], qbuf.at[piece], q_s.at[kind], q_r.at[kind], dev)

    q_sends = [q_copy(2, x, to_xo), q_copy(0, x, to_xr), q_copy(1, x, to_xl)]
    for cp in q_sends:
        cp.start()
    pl.when(c == KC)(k_begin)
    w_step(2)

    factor = (NOPE + ROPE) ** (-0.5) * LOG2E
    q_exchange = remote(qmine, qpart, qp_s.at[0], qp_r.at[0], partner)

    def make_q():
        q_copy(0, xl, to_xr).wait_recv()
        q_copy(1, xr, to_xl).wait_recv()
        q_copy(2, xo, to_xo).wait_recv()
        qf = qbuf[...].reshape(X * nq, T).astype(F32)
        scale = lax.rsqrt(jnp.mean(qf * qf, axis=0, keepdims=True) + EPS)
        qn = (qf * scale * qg_col[...]).astype(BF16)
        nope = dot_f32(wqn_v[...], qn, ((0,), (0,))) * factor
        qmine[: H * NOPE, :] = nope.astype(BF16)
        rope = dot_f32(wqr_v[...], qn, ((0,), (0,)))
        for i in range(H):
            r = turned(rope[i * ROPE : (i + 1) * ROPE], cs_scr[0], cs_scr[1]) * factor
            qmine[H * NOPE + i * ROPE : H * NOPE + (i + 1) * ROPE, :] = r.astype(BF16)
        q_exchange.start()

    def place_q():
        q_exchange.wait_recv()
        for i in range(H):
            p, e = divmod(i, 2)
            for src, at in ((qmine, 0), (qpart, T)):
                cols = slice(e * 2 * T + at, e * 2 * T + at + T)
                qz[p, e * NOPE : (e + 1) * NOPE, cols] = src[i * NOPE : (i + 1) * NOPE, :]
                qz[p, 2 * NOPE : 2 * NOPE + ROPE, cols] = src[H * NOPE + i * ROPE : H * NOPE + (i + 1) * ROPE, :]

    def keys(slot):
        lat = kvbuf[slot, :, c, :nk, :].reshape(X * nk, T).astype(F32)
        rope = kvbuf[slot, :, c, nk : nk + 2 * RX, :].astype(F32)[:, :RX].reshape(ROPE, T)
        return lat, rope

    def chunk(slot_a, slot_b):
        la, ra = keys(slot_a)
        lb, rb = keys(slot_b)
        lat = jnp.concatenate([la, lb], axis=1)
        scale = lax.rsqrt(jnp.mean(lat * lat, axis=0, keepdims=True) + EPS)
        gain = kvg_col[...]
        n = (lat * scale * jnp.concatenate([gain, gain], axis=1)).astype(BF16)
        kn = dot_f32(n, wkn_v[...], ((0,), (0,))).astype(BF16)
        rope = jnp.concatenate([ra, rb], axis=1)
        kr = jnp.transpose(jnp.concatenate([rope, jnp.zeros((128 - ROPE, 2 * T), F32)], axis=0)).astype(BF16)
        vt = dot_f32(wval_t[...], n).astype(BF16)
        for p in range(H // 2):
            kp = jnp.concatenate([kn[:, p * 128 : (p + 1) * 128], kr], axis=1)
            s = dot_f32(kp, qz[p])
            old = m_acc[p]
            new = jnp.maximum(old, jnp.max(s, axis=0, keepdims=True))
            m_acc[p] = new
            fade = jnp.exp2(old - new)
            w = jnp.exp2(s - new)
            l_acc[p] = l_acc[p] * fade + jnp.sum(w, axis=0, keepdims=True)
            wb = w.astype(BF16)
            for e in range(2):
                i = 2 * p + e
                cols = slice(e * 2 * T, (e + 1) * 2 * T)
                o_acc[i] = o_acc[i] * fade[:, cols] + dot_f32(vt[i * VALUE : (i + 1) * VALUE], wb[:, cols])

    def halo_copy(k, dev):
        rows = pl.ds(0, 8) if k == 1 else pl.ds(T - 8, 8)
        return remote(gated.at[rows], halo.at[k], h_s.at[k], h_r.at[k], dev)

    to_next, to_prev = {"sp": next_sp}, {"sp": prev_sp}

    def conv_gates():
        def got(i, _):
            w_p(lax.rem(z + i, Z)).wait_recv()
            return 0

        def all_in():
            lax.fori_loop(1, Z, got, 0)

        pl.when(c != WC)(all_in)

        def project(i):
            w = wbuf[i].reshape(D, wbuf.shape[-1])
            return (dot_f32(scaled[...], w) * rs_scr[:, 0:1]).astype(BF16).astype(F32)
        inner = project(2)
        value = project(0)
        gated[...] = (inner * value).astype(BF16).astype(F32)
        halo_copy(0, to_next).start()
        halo_copy(1, to_prev).start()
        yconv[...] = project(1)

    def spread(slot):
        k_x(slot, x, 0, to_xr).start()
        k_x(slot, x, 1, to_xl).start()

    def stop(j, way):
        slot = at(STRIDE * j if way else -STRIDE * j)
        k_near(slot, 0).wait_recv()
        pl.when(j < K)(lambda: k_far(slot, j, way).start())
        if way == 0:
            k_near(slot, 0).start()
            k_near(slot, 1).start()
        else:
            k_near(slot, 0).start()
            pl.when(j < K)(lambda: k_near(slot, 1).start())
        spread(slot)

    def leaf(slot):
        k_near(slot, 0).wait_recv()
        spread(slot)

    def relay_up(slot):
        k_x(slot, xl, 0, to_xr).wait_recv()
        k_x(slot, xl, 2, to_xr).start()

    def relay_dn(slot):
        k_x(slot, xr, 1, to_xl).wait_recv()
        k_x(slot, xr, 2, to_xl).start()

    def got_up(slot):
        k_x(slot, xr, 1, to_xl).wait_recv()
        k_x(slot, xo, 2, to_xr).wait_recv()

    def got_dn(slot):
        k_x(slot, xl, 0, to_xr).wait_recv()
        k_x(slot, xo, 2, to_xl).wait_recv()

    def pair(j, r):
        off = STRIDE * j + jnp.where(r == 0, 0, jnp.where(r == 1, -1, 1))
        own = off == HALF
        slot_a = at(-off)
        slot_b = jnp.where(own, z, at(off))

        def take():
            got_up(slot_a)
            pl.when(own)(lambda: got_up(slot_b))
            pl.when(jnp.logical_not(own))(lambda: got_dn(slot_b))
            k_hand(slot_a).start()
            k_hand(slot_b).start()

        def handed():
            k_hand(slot_a).wait_recv()
            k_hand(slot_b).wait_recv()

        pl.when(c == KC)(take)
        pl.when(c != KC)(handed)
        chunk(slot_a, slot_b)

    def transport(i):
        def stops_in():
            stop(i, 0)
            stop(i, 1)

        pl.when(i <= K)(stops_in)
        pl.when(i - 1 <= K)(lambda: leaves(i - 1, leaf, leaf))

        def relay_stops():
            relay_up(at(-STRIDE * (i - 1)))
            pl.when(i - 1 >= 1)(lambda: relay_dn(at(STRIDE * (i - 1))))

        pl.when(i - 1 <= K)(relay_stops)
        pl.when(jnp.logical_and(i - 2 >= 0, i - 2 <= K))(lambda: leaves(i - 2, relay_up, relay_dn))

    def step(i, _):
        pl.when(c == KC)(lambda: transport(i))
        w_step(i + 2)
        pl.when(i == 1)(make_q)
        pl.when(i == 2)(place_q)
        pl.when(i == K + 2)(conv_gates)

        def one(r, _):
            j = jnp.where(r == 0, i - 2, i - 3)
            here = jnp.logical_and(j >= jnp.where(r == 2, 0, 1), j <= K)
            pl.when(here)(lambda: pair(j, r))
            return 0

        lax.fori_loop(0, 3, one, 0)
        return 0

    lax.fori_loop(1, K + 4, step, 0)

    for i in range(H):
        p, e = divmod(i, 2)
        theirs = slice(e * 2 * T + T, (e + 1) * 2 * T)
        o_send[i * VALUE : (i + 1) * VALUE, :] = o_acc[i][:, T:]
        o_send[H * VALUE + i : H * VALUE + i + 1, :] = m_acc[p][:, theirs]
        o_send[H * VALUE + H + i : H * VALUE + H + i + 1, :] = l_acc[p][:, theirs]
    o_exchange = remote(o_send, o_recv, o_s.at[0], o_r.at[0], partner)
    o_exchange.start()

    halo_copy(0, to_next).wait_recv()
    halo_copy(1, to_prev).wait_recv()
    g = gated[...]
    row = lax.broadcasted_iota(jnp.int32, g.shape, 0)
    before = jnp.where(sp == 0, 0.0, halo[0, 7:8, :])
    after = jnp.where(sp == SP - 1, 0.0, halo[1, 0:1, :])
    g_before = jnp.where(row == 0, before, pltpu.roll(g, 1, 0))
    g_after = jnp.where(row == T - 1, after, pltpu.roll(g, T - 1, 0))
    taps = conv_kernel[...].astype(F32)
    conv = g_before * taps[0:1] + g * taps[1:2] + g_after * taps[2:3]
    y_conv = (yconv[...] * conv).astype(BF16)

    o_exchange.wait_recv()
    parts = []
    for i in range(H):
        p, e = divmod(i, 2)
        ours = slice(e * 2 * T, e * 2 * T + T)
        m1 = m_acc[p][:, ours]
        m2 = o_recv[H * VALUE + i : H * VALUE + i + 1, :]
        top = jnp.maximum(m1, m2)
        a1, a2 = jnp.exp2(m1 - top), jnp.exp2(m2 - top)
        total = a1 * l_acc[p][:, ours] + a2 * o_recv[H * VALUE + H + i : H * VALUE + H + i + 1, :]
        summed = a1 * o_acc[i][:, :T] + a2 * o_recv[i * VALUE : (i + 1) * VALUE, :]
        parts.append(summed / total)
    y_attn = jnp.transpose(jnp.concatenate(parts, axis=0)).astype(BF16)
    y = jnp.concatenate([y_conv, y_attn], axis=1)
    for cp in out_cp:
        cp.wait()
    for rel, dev in ((2, to_xo), (1, to_xr), (3, to_xl), (0, None)):
        dest = lax.rem(x + rel, X)
        cols = pl.ds(pl.multiple_of(dest * DX, DX), DX)
        rs_send[rel] = dot_f32(y, wout[:, cols]).astype(BF16)
        if dev is not None:
            remote(rs_send.at[rel], rs_recv.at[rel - 1], r_s.at[rel - 1], r_r.at[rel - 1], dev).start()
    for cp in tok_sends + [tok_copy(4, xl, lo, to_xr, False), tok_copy(5, xr, hi, to_xl, False)]:
        cp.wait_send()
    for cp in q_sends + [q_exchange, halo_copy(0, to_next), halo_copy(1, to_prev), o_exchange]:
        cp.wait_send()

    w_own(c).wait_send()

    def w_sent(j, _):
        for core in (0, 1):
            for way in (0, 1):
                pl.when(j < K)(lambda way=way, core=core: w_far(z, j, way, core).wait_send())
                w_near(at(-STRIDE * j), way, core).wait_send()

            def back(core=core):
                w_near(at(STRIDE * j), 0, core).wait_send()
                pl.when(j < K)(lambda: w_near(at(STRIDE * j), 1, core).wait_send())

            pl.when(j >= 1)(back)
        return 0

    def w_handed(i, _):
        w_p(lax.rem(z + i, Z)).wait_send()
        return 0

    def w_all():
        lax.fori_loop(0, K + 1, w_sent, 0)
        lax.fori_loop(1, Z, w_handed, 0)

    pl.when(c == WC)(w_all)

    def k_sent(j, _):
        for way in (0, 1):
            pl.when(j < K)(lambda way=way: k_far(z, j, way).wait_send())
        k_near(at(-STRIDE * j), 0).wait_send()
        k_near(at(-STRIDE * j), 1).wait_send()

        def back():
            k_near(at(STRIDE * j), 0).wait_send()
            pl.when(j < K)(lambda: k_near(at(STRIDE * j), 1).wait_send())

        pl.when(j >= 1)(back)
        return 0

    def sent_slots(s, _):
        for kind, dev in ((0, to_xr), (1, to_xl), (2, to_xr)):
            k_x(s, x, kind, dev).wait_send()
        k_hand(s).wait_send()
        return 0

    def k_all():
        lax.fori_loop(0, K + 1, k_sent, 0)
        lax.fori_loop(0, Z, sent_slots, 0)

    pl.when(c == KC)(k_all)
    pl.when(c != KC)(k_own.wait_send)

    total = rs_send[0].astype(F32)
    r_copies = [
        remote(rs_send.at[rel], rs_recv.at[rel - 1], r_s.at[rel - 1], r_r.at[rel - 1], dev)
        for rel, dev in ((1, to_xr), (3, to_xl), (2, to_xo))
    ]
    for rel, cp in zip((1, 3, 2), r_copies):
        cp.wait_recv()
        total += rs_recv[rel - 1].astype(F32)
    out[...] = total.astype(BF16)
    for cp in r_copies:
        cp.wait_send()


def solution(mesh):
    SP, X = mesh.shape["sp"], mesh.shape["tp"]

    def per_device(
        tokens, mix_gain, wv, wo, wi, conv_kernel, wqd, wkvd, wrk, q_gain, kv_gain,
        wqn, wqr, wkn, wval, woc, woa,
    ):
        T, DX = tokens.shape
        D = DX * X
        Z = SP // 2
        R, CC = wv.shape
        H = wqn.shape[1] // NOPE
        nk, nq = wkvd.shape[1], wqd.shape[1]
        K = (Z // 2 - 1) // STRIDE
        RX = ROPE // X
        anyspace = pl.BlockSpec(memory_space=pl.ANY)
        vmem = pl.BlockSpec(memory_space=pltpu.VMEM)
        V = pltpu.VMEM
        DMA = pltpu.SemaphoreType.DMA
        scratch = [
            V((3, Z, 2, R, CC), BF16),
            V((X, T, DX), BF16),
            V((T, D), BF16),
            V(wqd.shape, BF16),
            V((128, D), BF16),
            V(wqn.shape, BF16), V(wqr.shape, BF16), V(wkn.shape, BF16), V(wval.shape, BF16),
            V((wval.shape[1], wval.shape[0]), BF16),
            V((woc.shape[0] + woa.shape[0], woc.shape[1]), BF16),
            V((X, nq, T), BF16),
            V((H * (NOPE + ROPE), T), BF16), V((H * (NOPE + ROPE), T), BF16),
            V((H // 2, 256, 4 * T), BF16),
            V((Z, X, 2, nk + 2 * RX, T), BF16), V((nk + 2 * RX, T), BF16),
            V((ROPE, T), F32), V((2, ROPE, T), F32),
            V((nq * X, 128), F32), V((nk * X, 128), F32),
            V((T, 128), F32),
            V((H, VALUE, 2 * T), F32), V((H // 2, 1, 4 * T), F32), V((H // 2, 1, 4 * T), F32),
            V((H * VALUE + 2 * H, T), F32), V((H * VALUE + 2 * H, T), F32),
            V((T, CC), F32), V((2, 8, CC), F32), V((T, CC), F32),
            V((X, T, DX), BF16), V((X - 1, T, DX), BF16),
            DMA((13,)),
            DMA((6,)), DMA((6,)),
            DMA((3,)), DMA((3,)), DMA((1,)), DMA((1,)),
            DMA((2, K)), DMA((Z, 2)), DMA((1,)), DMA((1,)), DMA((Z,)), DMA((Z,)), DMA((Z,)), DMA((Z, 3)), DMA((Z, 3)),
            DMA((2, K, 2)), DMA((Z, 2, 2)), DMA((Z, 2)), DMA((Z,)), DMA((Z,)), DMA((1,)), DMA((1,)),
            DMA((1,)), DMA((1,)), DMA((2,)), DMA((2,)), DMA((3,)), DMA((3,)),
        ]
        return pl.pallas_call(
            functools.partial(kernel, SP, X),
            out_shape=jax.ShapeDtypeStruct((T, DX), BF16),
            in_specs=[anyspace, vmem, anyspace, anyspace, anyspace, vmem, anyspace, anyspace, anyspace,
                      vmem, vmem] + [anyspace] * 6,
            out_specs=vmem,
            scratch_shapes=scratch,
            compiler_params=pltpu.CompilerParams(
                collective_id=0, has_side_effects=True, vmem_limit_bytes=56 * 1024 * 1024
            ),
        )(
            tokens, mix_gain.reshape(1, -1), wv, wo, wi, conv_kernel, wqd, wkvd.T, wrk.T,
            q_gain.reshape(1, -1), kv_gain.reshape(1, -1), wqn, wqr, wkn, wval, woc, woa,
        )

    placed = (
        P(("grp", "sp"), "tp"),
        P(),
        P("sp", "tp"),
        P("sp", "tp"),
        P("sp", "tp"),
        P(None, "tp"),
        P(None, "tp"),
        P(None, "tp"),
        P(),
        P(),
        P(),
        P(None, "tp"),
        P(None, "tp"),
        P(None, "tp"),
        P(None, "tp"),
        P("tp", None),
        P("tp", None),
    )
    return jax.shard_map(
        per_device, mesh=mesh, in_specs=placed, out_specs=P(("grp", "sp"), "tp"), check_vma=False
    )
```
